512 devices in a mesh: ep: 32 (over z, x), tp: 16 (over y, core).
Axes of the slice: x: 4, y: 8, z: 8, core: 2. Of those that a mesh axis runs over, the one named last changes fastest.
Arguments:
- tokens: bfloat16 [8192, 2048], P('ep')
- norm_gain: float32 [2048], replicated, may hold values from 0.1 to 1.9
- chosen: int32 [32, 1024], replicated, may hold values from 0 to 8191, as said below
- route_weight: float32 [32, 1024], P('ep'), may hold values from 0.2 to 1
- gate_weight: bfloat16 [32, 2048, 4096], P('ep', None, 'tp'), may hold values from -0.125 to 0.125
- up_weight: bfloat16 [32, 2048, 4096], P('ep', None, 'tp'), may hold values from -0.125 to 0.125
- down_weight: bfloat16 [32, 4096, 2048], P('ep', 'tp'), may hold values from -0.09375 to 0.09375
Outputs:
- combined: bfloat16 [8192, 2048], P('ep', 'tp')
The draws below stay inside these ranges and needn't reach their ends.
Inputs may be any that keep to these rules, and one draw needn't show every extreme that they name: Each row of chosen lists 1024 distinct token numbers in ascending order. Of the 256 consecutive tokens of one index of ep, a row holds at most 48, and every draw has rows that hold exactly 48 of them.
All inputs are finite; a program needn't handle non-finite values.
Results may differ from the reference program's by a relative error of at most 0.02.
Values may be sent and summed in bfloat16 or wider, within the bound.
No kernel may reach another device: no remote copies, remote signals or barrier semaphores. Data moves between devices by JAX's collectives and lax.ppermute only.
A program may use at most 64 MiB of HBM per device.

```python
import math
import jax
import jax.numpy as jnp
from jax import lax

D = 2048
FF = 4096
TOK_DEV = 256
EXPERTS = 32
TOKENS = 8192
CAP = 1024
FF_BLK = 256
N_TP = 16


def draw_tokens(key, part):
    keys = jax.random.split(jax.random.fold_in(key, 11), 3)
    row_scale = jnp.exp(jax.random.uniform(keys[0], (TOKENS, 1), jnp.float32, 0.0, math.log(10.0)))
    col_scale = jnp.exp(jax.random.uniform(keys[1], (1, D), jnp.float32, 0.0, math.log(10.0)))
    values = jax.random.normal(keys[2], (TOKENS, D), jnp.float32)
    return (values * row_scale * col_scale / 3.0).astype(jnp.bfloat16)


def draw_chosen(key, part):
    share = TOK_DEV // 8
    pairs = EXPERTS // 2
    steps = jnp.arange(pairs, dtype=jnp.int32)
    spread = share // 2 * steps // max(pairs - 1, 1)
    base = jnp.stack([share + spread, share - spread], axis=1).reshape(EXPERTS)
    expert_keys = jax.random.split(jax.random.fold_in(key, 23), EXPERTS)

    def one_expert(expert_key):
        order_key, rank_key = jax.random.split(expert_key)
        counts = base[jax.random.permutation(order_key, EXPERTS)]
        block_keys = jax.random.split(rank_key, EXPERTS)
        ranks = jax.vmap(lambda block_key: jax.random.permutation(block_key, TOK_DEV))(block_keys)
        picked = (ranks < counts[:, None]).reshape(TOKENS).astype(jnp.int32)
        order = jnp.argsort(1 - picked, stable=True)
        return order[:CAP].astype(jnp.int32)
    return jax.vmap(one_expert)(expert_keys)


def steps_of(stream_key, extent, cuts, least, top_value):
    def one(dim, blocks):
        heights = jax.random.uniform(jax.random.fold_in(jax.random.fold_in(stream_key, 6), dim), (blocks,), jnp.float32, least / len(cuts), top_value / len(cuts))
        return jnp.repeat(jnp.exp(heights), extent[dim] // blocks).reshape((-1,) + (1,) * (len(extent) - dim - 1))

    gain = one(*cuts[0])
    for cut in cuts[1:]:
        gain = gain * one(*cut)
    return gain


def scatter_about(stream_key, shape, width, reach, pieces=(), kind=jnp.bfloat16):
    array = width * jax.random.normal(stream_key, shape, jnp.float32)
    if pieces:
        array = array * steps_of(stream_key, shape, pieces, -0.22, 0.18)
    return jnp.clip(array, -reach, reach).astype(kind)


def setup_inputs(seed: int = 0) -> dict:
    key_list = jax.random.split(jax.random.key(seed), 8)
    return {
        "tokens": draw_tokens(jax.random.fold_in(key_list[7], 71), 0),
        "norm_gain": jnp.clip(1.0 + 0.18 * jax.random.normal(key_list[1], (D,), jnp.float32), 0.1, 1.9),
        "chosen": draw_chosen(jax.random.fold_in(key_list[7], 71), 0),
        "route_weight": jnp.clip(0.2 + 0.8 * jax.random.uniform(key_list[3], (EXPERTS, CAP), jnp.float32) ** steps_of(key_list[3], (EXPERTS, CAP), ((0, 32),), -0.2, 0.2), 0.2, 1.0),
        "gate_weight": scatter_about(key_list[4], (EXPERTS, D, FF), D ** -0.5, 0.125, ((0, 32), (2, 16))),
        "up_weight": scatter_about(key_list[5], (EXPERTS, D, FF), D ** -0.5, 0.125, ((0, 32), (2, 16))),
        "down_weight": scatter_about(key_list[6], (EXPERTS, FF, D), FF ** -0.5, 0.09375, ((0, 32), (1, 16))),
    }


def normalize(tokens, norm_gain):
    values = tokens.astype(jnp.float32)
    scale = lax.rsqrt(lax.optimization_barrier(jnp.mean(values * values, axis=-1, keepdims=True)) + 1e-06)
    return (values * scale * norm_gain[None, :]).astype(jnp.bfloat16)

def reference(tokens, norm_gain, chosen, route_weight, gate_weight, up_weight, down_weight):
    normed = normalize(tokens, norm_gain)

    def expert_step(combined, inputs):
        token_ids, weights, gate_mat, up_mat, down_mat = inputs
        expert_rows = normed[token_ids]
        gate_pre = jnp.dot(expert_rows, gate_mat, preferred_element_type=jnp.float32)
        up_pre = jnp.dot(expert_rows, up_mat, preferred_element_type=jnp.float32)
        hidden = (jax.nn.silu(gate_pre) * up_pre).astype(jnp.bfloat16)
        hidden_blocks = hidden.reshape(CAP, N_TP, FF_BLK).astype(jnp.float32)
        down_blocks = down_mat.reshape(N_TP, FF_BLK, D).astype(jnp.float32)
        partial_value = jnp.einsum('cnf,nfd->ncd', hidden_blocks, down_blocks).astype(jnp.bfloat16)
        partial_value = lax.optimization_barrier(partial_value)
        summed = lax.optimization_barrier(jnp.sum(partial_value.astype(jnp.float32), axis=0))
        weighted = (weights[:, None] * summed).astype(jnp.bfloat16)
        combined = combined.at[token_ids].add(weighted.astype(jnp.float32))
        return (combined, None)
    start_total = jnp.zeros((TOKENS, D), jnp.float32)
    combined, _ = lax.scan(expert_step, start_total, (chosen, route_weight, gate_weight, up_weight, down_weight))
    return combined.astype(jnp.bfloat16)
```

```python
import jax
import jax.numpy as jnp
from jax import lax
from jax.sharding import Mesh
from jax.sharding import PartitionSpec as P

BF16 = jnp.bfloat16
F32 = jnp.float32


def shift(n, k):
    return [(i, (i + k) % n) for i in range(n)]


def dot(a, b, dims=(((1,), (0,)), ((), ()))):
    return lax.dot_general(a, b, dims, preferred_element_type=F32)


def shards(tokens, norm_gain, chosen, route_weight, gate_weight, up_weight, down_weight):
    tok_rows, width = tokens.shape
    experts, capacity = chosen.shape
    p = lax.axis_index("ep")
    y = lax.axis_index("y")
    c = lax.axis_index("c")
    q = y % 4
    h = y // 4
    block = width // 16
    quarter = width // 4
    half_rows = capacity // 2
    quart_rows = half_rows // 2
    slots = 3 * tok_rows // 32
    mate = [(0, 1), (1, 0)]

    def quarter_of(x, j, dim):
        shape = x.shape[:dim] + (2, 4, 2 * block) + x.shape[dim + 1 :]
        picked = lax.dynamic_index_in_dim(x.reshape(shape), j % 4, dim + 1, keepdims=False)
        return picked.reshape(x.shape[:dim] + (quarter,) + x.shape[dim + 1 :])

    first_token = p * tok_rows
    run_start = jnp.sum((chosen < first_token).astype(jnp.int32), axis=1)
    run_end = jnp.sum((chosen < first_token + tok_rows).astype(jnp.int32), axis=1)
    first = run_start + ((run_start + c) % 2)
    slot_rank = first[:, None] + 2 * jnp.arange(slots, dtype=jnp.int32)[None, :]
    rank = jnp.arange(capacity, dtype=jnp.int32)
    slot_token = jnp.sum(
        jnp.where(rank[None, None, :] == slot_rank[:, :, None], chosen[:, None, :], 0), axis=2
    )
    slot_local = jnp.where(slot_rank < run_end[:, None], slot_token - first_token, tok_rows)
    pick_token = (
        slot_local[:, :, None] == jnp.arange(tok_rows, dtype=jnp.int32)[None, None, :]
    ).astype(BF16).reshape(experts * slots, tok_rows)

    mine = lax.dynamic_index_in_dim(chosen, p, 0, keepdims=False)
    edges = jnp.arange(experts + 1, dtype=jnp.int32) * tok_rows
    src_edge = jnp.sum((mine[None, :] < edges[:, None]).astype(jnp.int32), axis=1)
    k_edge = (src_edge - c + 1) // 2
    k_slot = k_edge[:-1, None] + jnp.arange(slots, dtype=jnp.int32)[None, :]
    k_slot = jnp.where(k_slot < k_edge[1:, None], k_slot, half_rows)
    pick_row = (
        k_slot[:, :, None] == jnp.arange(half_rows, dtype=jnp.int32)[None, None, :]
    ).astype(BF16).reshape(experts * slots, half_rows)
    my_weight = lax.dynamic_index_in_dim(
        route_weight.reshape(half_rows, 2), c, 1, keepdims=True
    )

    values = tokens.astype(F32)
    scale = lax.rsqrt(jnp.mean(values * values, axis=-1, keepdims=True) + 1e-06)
    my_gain = quarter_of(norm_gain, q, 0)
    normed = (quarter_of(tokens, q, 1).astype(F32) * scale * my_gain[None, :]).astype(BF16)

    sent = dot(pick_token, normed).astype(BF16).reshape(experts, slots, quarter)
    got = lax.all_to_all(sent, "ep", 0, 0, tiled=True).reshape(experts * slots, quarter)
    own = dot(pick_row, got, (((0,), (0,)), ((), ()))).astype(BF16)

    def around(x_up, x_down, x_up2, x_down2):
        return (
            lax.ppermute(x_up, "y", shift(8, 1)),
            lax.ppermute(x_down, "y", shift(8, -1)),
            lax.ppermute(x_up2, "y", shift(8, 2)),
            lax.ppermute(x_down2, "y", shift(8, -2)),
        )

    below, above, far_a, far_b = around(own, own, own[:quart_rows], own[quart_rows:])
    far = jnp.concatenate([far_a, far_b], axis=0)

    gate_w, up_w, down_w = gate_weight[0], up_weight[0], down_weight[0]
    gate_w, up_w, down_w, own = lax.optimization_barrier((gate_w, up_w, down_w, own))
    gate_m = lax.ppermute(gate_w, "c", mate)
    up_m = lax.ppermute(up_w, "c", mate)
    down_m = lax.ppermute(down_w, "c", mate)

    def hidden_of(gate_mat, up_mat):
        pre = [
            sum(dot(x, quarter_of(w, q + j, 0)) for x, j in ((own, 0), (below, 3), (above, 1), (far, 2)))
            for w in (gate_mat, up_mat)
        ]
        return (jax.nn.silu(pre[0]) * pre[1]).astype(BF16)

    hid = hidden_of(gate_w, up_w)
    hid_m = hidden_of(gate_m, up_m)

    def out_of(j):
        return dot(hid, quarter_of(down_w, q + j, 1)) + dot(hid_m, quarter_of(down_m, q + j, 1))

    out_far = out_of(2).astype(BF16)
    r_below, r_above, r_far_a, r_far_b = around(
        out_of(1).astype(BF16), out_of(3).astype(BF16), out_far[:quart_rows], out_far[quart_rows:]
    )
    total = out_of(0) + r_below.astype(F32) + r_above.astype(F32)
    total = total + jnp.concatenate([r_far_a, r_far_b], axis=0).astype(F32)
    weighted = (my_weight * total).astype(BF16)

    back = dot(pick_row, weighted).astype(BF16).reshape(experts, slots, quarter)
    returned = lax.all_to_all(back, "ep", 0, 0, tiled=True).reshape(experts * slots, quarter)
    part = dot(pick_token, returned, (((0,), (0,)), ((), ()))).reshape(tok_rows, 2, 2, block)

    def cell(i, j):
        row = lax.dynamic_index_in_dim(part, i % 2, 1, keepdims=False)
        return lax.dynamic_index_in_dim(row, j % 2, 1, keepdims=False)

    opposite = shift(8, 4)
    both = [((i, j), ((i + 4) % 8, 1 - j)) for i in range(8) for j in range(2)]
    both = [(2 * a + b, 2 * d + e) for (a, b), (d, e) in both]
    from_mate = lax.ppermute(cell(h, c + 1).astype(BF16), "c", mate)
    from_far = lax.ppermute(cell(h + 1, c).astype(BF16), "y", opposite)
    from_both = lax.ppermute(cell(h + 1, c + 1).astype(BF16), ("y", "c"), both)
    combined = cell(h, c) + from_mate.astype(F32) + from_far.astype(F32) + from_both.astype(F32)
    return combined.astype(BF16)


def solution(mesh):
    finer = Mesh(mesh.devices.reshape(mesh.shape["ep"], 8, 2), ("ep", "y", "c"))
    tp = ("y", "c")
    in_specs = (
        P("ep", None),
        P(),
        P(),
        P("ep", None),
        P("ep", None, tp),
        P("ep", None, tp),
        P("ep", tp, None),
    )
    return jax.shard_map(
        shards, mesh=finer, in_specs=in_specs, out_specs=P("ep", tp), check_vma=False
    )
```

```python
import functools

import jax
import jax.numpy as jnp
from jax import lax
from jax.experimental import pallas as pl
from jax.experimental.pallas import tpu as pltpu
from jax.sharding import Mesh
from jax.sharding import PartitionSpec as P


BF16 = jnp.bfloat16
F32 = jnp.float32
I32 = jnp.int32
OVER_ROWS = (((0,), (0,)), ((), ()))


def shift(n, k):
    return [(i, (i + k) % n) for i in range(n)]


def dot(a, b, dims=(((1,), (0,)), ((), ()))):
    return lax.dot_general(a, b, dims, preferred_element_type=F32)


def dispatch_kernel(slots, where_ref, tokens_ref, gain_ref, chosen_ref, pick_ref, sent_ref, held):
    tok_rows, width = tokens_ref.shape
    experts, capacity = chosen_ref.shape
    first_token, parity, q = where_ref[0], where_ref[1], where_ref[2]
    chosen = chosen_ref[...]
    run_start = jnp.sum((chosen < first_token).astype(I32), axis=1, keepdims=True)
    run_end = jnp.sum((chosen < first_token + tok_rows).astype(I32), axis=1, keepdims=True)
    first = run_start + ((run_start + parity) & 1)
    rank = lax.broadcasted_iota(I32, (slots, capacity), 1)
    step = 2 * lax.broadcasted_iota(I32, (slots, capacity), 0)
    ahead = rank - step
    slot = 2 * lax.broadcasted_iota(I32, (slots, 1), 0)
    column = lax.broadcasted_iota(I32, (slots, tok_rows), 1)
    for e in range(experts):
        start = first[e : e + 1, :]
        token = jnp.sum(
            jnp.where(ahead == start, chosen[e : e + 1, :], 0), axis=1, keepdims=True
        )
        local = jnp.where(slot + start < run_end[e : e + 1, :], token - first_token, tok_rows)
        held[e * slots : (e + 1) * slots, :] = (column == local).astype(F32)
    values = tokens_ref[...].astype(F32)
    scale = lax.rsqrt(jnp.mean(values * values, axis=-1, keepdims=True) + 1e-06)
    piece = width // 8
    pick = held[...].astype(BF16)
    pick_ref[...] = pick
    for s in range(2):
        at = pl.multiple_of(s * (width // 2) + q * piece, piece)
        part = tokens_ref[:, pl.ds(at, piece)].astype(F32)
        normed = (part * scale * gain_ref[:, pl.ds(at, piece)]).astype(BF16)
        sent_ref[:, s * piece : (s + 1) * piece] = jnp.dot(
            pick, normed, preferred_element_type=F32
        ).astype(BF16)


def dispatch(tokens, norm_gain, chosen, where, slots):
    experts = chosen.shape[0]
    tok_rows, width = tokens.shape
    rows = experts * slots
    vmem = pl.BlockSpec(memory_space=pltpu.VMEM)
    return pl.pallas_call(
        functools.partial(dispatch_kernel, slots),
        out_shape=(
            jax.ShapeDtypeStruct((rows, tok_rows), BF16),
            jax.ShapeDtypeStruct((rows, width // 4), BF16),
        ),
        in_specs=[pl.BlockSpec(memory_space=pltpu.SMEM), vmem, vmem, vmem],
        out_specs=(vmem, vmem),
        scratch_shapes=[pltpu.VMEM((rows, tok_rows), F32)],
        compiler_params=pltpu.CompilerParams(vmem_limit_bytes=12 << 20),
    )(where, tokens, norm_gain.reshape(1, width), chosen)


def weight_rows(ref, j):
    return ref[:, pl.ds(j, 1), :, :].reshape(2 * ref.shape[2], ref.shape[3])


def near_kernel(q_ref, own, below_a, below_b, above_a, above_b, *refs):
    weights, totals = refs[:4], refs[4:]
    q = q_ref[0]
    mid = below_a.shape[0]
    for w_ref, total in zip(weights, totals):
        w_own = weight_rows(w_ref, q)
        w_below = weight_rows(w_ref, (q + 3) & 3)
        w_above = weight_rows(w_ref, (q + 1) & 3)
        for r, (below, above) in enumerate(((below_a, above_a), (below_b, above_b))):
            rows = slice(r * mid, (r + 1) * mid)
            total[rows, :] = (
                dot(own[rows, :], w_own) + dot(below[...], w_below) + dot(above[...], w_above)
            )


def far_kernel(
    q_ref, far_a, far_b, t_gate, t_up, t_gate_m, t_up_m, gate, up, gate_m, up_m, down, down_m,
    far_out_a, far_out_b, up_out_a, up_out_b, down_out_a, down_out_b, own_out,
):
    q = q_ref[0]
    mid = far_a.shape[0]
    piece = gate.shape[2]
    j_far = (q + 2) & 3
    w = [weight_rows(ref, j_far) for ref in (gate, up, gate_m, up_m)]
    hid = []
    for r, far in enumerate((far_a, far_b)):
        rows = slice(r * mid, (r + 1) * mid)
        x = far[...]
        pre = [t[rows, :] + dot(x, m) for t, m in zip((t_gate, t_up, t_gate_m, t_up_m), w)]
        hid.append(
            [
                (pre[2 * k] / (1.0 + jnp.exp(-pre[2 * k])) * pre[2 * k + 1]).astype(BF16)
                for k in range(2)
            ]
        )
    targets = (
        ((q + 2) & 3, (far_out_a, far_out_b)),
        ((q + 1) & 3, (up_out_a, up_out_b)),
        ((q + 3) & 3, (down_out_a, down_out_b)),
        (q, (own_out.at[0:mid, :], own_out.at[mid : 2 * mid, :])),
    )
    for j, outs in targets:
        for s in range(2):
            at = pl.multiple_of((s * 4 + j) * piece, piece)
            d_own = down[:, pl.ds(at, piece)]
            d_mate = down_m[:, pl.ds(at, piece)]
            for r in range(2):
                value = dot(hid[r][0], d_own) + dot(hid[r][1], d_mate)
                outs[r][:, s * piece : (s + 1) * piece] = value.astype(outs[r].dtype)


def call_vmem(kernel, out_shape, flops, q, *arrays):
    vmem = pl.BlockSpec(memory_space=pltpu.VMEM)
    return pl.pallas_call(
        kernel,
        out_shape=out_shape,
        in_specs=[pl.BlockSpec(memory_space=pltpu.SMEM)] + [vmem] * len(arrays),
        out_specs=tuple(vmem for _ in out_shape),
        cost_estimate=pl.CostEstimate(flops=flops, bytes_accessed=8 << 20, transcendentals=0),
        compiler_params=pltpu.CompilerParams(vmem_limit_bytes=20 << 20),
    )(q, *arrays)


def shards(tokens, norm_gain, chosen, route_weight, gate_weight, up_weight, down_weight):
    tok_rows, width = tokens.shape
    experts, capacity = chosen.shape
    p = lax.axis_index("ep")
    y = lax.axis_index("y")
    c = lax.axis_index("c")
    q = lax.bitwise_and(y, 3)
    h = lax.shift_right_logical(y, 2)
    block = width // 16
    piece = 2 * block
    quarter = 2 * piece
    half_rows = capacity // 2
    mid = half_rows // 2
    slots = 3 * tok_rows // 32
    mate = [(0, 1), (1, 0)]
    up, down = shift(8, 1), shift(8, -1)

    where = jnp.stack([p * tok_rows, c, q]).astype(I32)
    pick_token, sent = dispatch(tokens, norm_gain, chosen, where, slots)
    got = lax.all_to_all(sent.reshape(experts, slots, quarter), "ep", 0, 0, tiled=True)
    got = got.reshape(experts * slots, quarter)

    gate_w, up_w, down_w, _ = lax.optimization_barrier(
        (gate_weight[0], up_weight[0], down_weight[0], sent)
    )
    gate_m = lax.ppermute(gate_w, "c", mate)
    up_m = lax.ppermute(up_w, "c", mate)
    down_m = lax.ppermute(down_w, "c", mate)

    mine = lax.dynamic_index_in_dim(chosen, p, 0, keepdims=False)
    edges = jnp.arange(experts + 1, dtype=I32) * tok_rows
    src_edge = jnp.sum((mine[None, :] < edges[:, None]).astype(I32), axis=1)
    k_edge = lax.shift_right_logical(src_edge - c + 1, 1)
    k_slot = k_edge[:-1, None] + jnp.arange(slots, dtype=I32)[None, :]
    k_slot = jnp.where(k_slot < k_edge[1:, None], k_slot, half_rows)
    pick_row = (
        k_slot[:, :, None] == jnp.arange(half_rows, dtype=I32)[None, None, :]
    ).astype(BF16).reshape(experts * slots, half_rows)
    my_weight = lax.dynamic_index_in_dim(
        route_weight.reshape(half_rows, 2), c, 1, keepdims=True
    )

    own = dot(pick_row, got, OVER_ROWS).astype(BF16)
    below_a = lax.ppermute(own[:mid], "y", up)
    above_b = lax.ppermute(own[mid:], "y", down)
    below_b = lax.ppermute(own[mid:], "y", up)
    above_a = lax.ppermute(own[:mid], "y", down)
    far_a = lax.ppermute(below_a, "y", up)
    far_b = lax.ppermute(above_b, "y", down)
    def view(w):
        return w.reshape(2, 4, piece, w.shape[1])

    gates = [view(w) for w in (gate_w, up_w, gate_m, up_m)]
    units = gate_w.shape[1]
    q_one = q.astype(I32).reshape(1)
    totals = call_vmem(
        near_kernel,
        [jax.ShapeDtypeStruct((half_rows, units), F32)] * 4,
        2 * half_rows * 3 * quarter * 4 * units,
        q_one, own, below_a, below_b, above_a, above_b, *gates,
    )
    part_shape = jax.ShapeDtypeStruct((mid, quarter), BF16)
    wide_shape = jax.ShapeDtypeStruct((mid, quarter), F32)
    far_out_a, far_out_b, up_out_a, up_out_b, down_out_a, down_out_b, own_out = call_vmem(
        far_kernel,
        [part_shape, part_shape, wide_shape, part_shape, part_shape, wide_shape,
         jax.ShapeDtypeStruct((half_rows, quarter), F32)],
        2 * half_rows * (quarter * 4 * units + 2 * units * width),
        q_one, far_a, far_b, *totals, *gates, down_w, down_m,
    )
    r_far_a = lax.ppermute(far_out_a, "y", up)
    r_far_b = lax.ppermute(far_out_b, "y", down)
    r_below_b = lax.ppermute(up_out_b, "y", up)
    r_above_a = lax.ppermute(down_out_a, "y", down)
    r_below_a = lax.ppermute((up_out_a + r_far_a.astype(F32)).astype(BF16), "y", up)
    r_above_b = lax.ppermute((down_out_b + r_far_b.astype(F32)).astype(BF16), "y", down)
    total = own_out + jnp.concatenate([r_below_a, r_below_b], axis=0).astype(F32)
    total = total + jnp.concatenate([r_above_a, r_above_b], axis=0).astype(F32)
    weighted = (my_weight * total).astype(BF16)

    back = dot(pick_row, weighted).astype(BF16).reshape(experts, slots, quarter)
    returned = lax.all_to_all(back, "ep", 0, 0, tiled=True).reshape(experts * slots, quarter)
    part = dot(pick_token, returned, OVER_ROWS)

    both = [
        lax.dynamic_slice_in_dim(part, s * piece + (1 - c) * block, block, 1) for s in range(2)
    ]
    kept = [lax.dynamic_slice_in_dim(part, s * piece + c * block, block, 1) for s in range(2)]
    theirs = lax.ppermute(jnp.concatenate(both, axis=1).astype(BF16), "c", mate)
    mine_sum = [kept[s] + theirs[:, s * block : (s + 1) * block].astype(F32) for s in range(2)]
    lower = h == 0
    sent_far = jnp.where(lower, mine_sum[1], mine_sum[0]).astype(BF16)
    from_far = lax.ppermute(sent_far, "y", shift(8, 4))
    combined = jnp.where(lower, mine_sum[0], mine_sum[1]) + from_far.astype(F32)
    return combined.astype(BF16)


def solution(mesh):
    finer = Mesh(mesh.devices.reshape(mesh.shape["ep"], 8, 2), ("ep", "y", "c"))
    tp = ("y", "c")
    in_specs = (
        P("ep", None),
        P(),
        P(),
        P("ep", None),
        P("ep", None, tp),
        P("ep", None, tp),
        P("ep", tp, None),
    )
    return jax.shard_map(
        shards, mesh=finer, in_specs=in_specs, out_specs=P("ep", tp), check_vma=False
    )
```

```python
import functools

import jax
import jax.numpy as jnp
from jax import lax
from jax.experimental import pallas as pl
from jax.experimental.pallas import tpu as pltpu
from jax.sharding import Mesh
from jax.sharding import PartitionSpec as P


BF16 = jnp.bfloat16
F32 = jnp.float32
I32 = jnp.int32
OVER_ROWS = (((0,), (0,)), ((), ()))


def shift(n, k):
    return [(i, (i + k) % n) for i in range(n)]


def dot(a, b, dims=(((1,), (0,)), ((), ()))):
    return lax.dot_general(a, b, dims, preferred_element_type=F32)


def dispatch_kernel(
    slots, where_ref, tokens_in, gain_in, chosen_in, pick_ref, sent_ref,
    held, tokens_ref, gain_ref, chosen_ref, sems,
):
    copies = [
        pltpu.make_async_copy(chosen_in, chosen_ref, sems.at[0]),
        pltpu.make_async_copy(tokens_in, tokens_ref, sems.at[1]),
        pltpu.make_async_copy(gain_in, gain_ref, sems.at[2]),
    ]
    for copy in copies:
        copy.start()
    copies[0].wait()
    tok_rows, width = tokens_ref.shape
    experts, capacity = chosen_ref.shape
    first_token, parity, q = where_ref[0], where_ref[1], where_ref[2]
    chosen = chosen_ref[...]
    run_start = jnp.sum((chosen < first_token).astype(I32), axis=1, keepdims=True)
    run_end = jnp.sum((chosen < first_token + tok_rows).astype(I32), axis=1, keepdims=True)
    first = run_start + ((run_start + parity) & 1)
    rank = lax.broadcasted_iota(I32, (slots, capacity), 1)
    step = 2 * lax.broadcasted_iota(I32, (slots, capacity), 0)
    ahead = rank - step
    slot = 2 * lax.broadcasted_iota(I32, (slots, 1), 0)
    column = lax.broadcasted_iota(I32, (slots, tok_rows), 1)
    for e in range(experts):
        start = first[e : e + 1, :]
        token = jnp.sum(
            jnp.where(ahead == start, chosen[e : e + 1, :], 0), axis=1, keepdims=True
        )
        local = jnp.where(slot + start < run_end[e : e + 1, :], token - first_token, tok_rows)
        held[e * slots : (e + 1) * slots, :] = (column == local).astype(F32)
    copies[1].wait()
    copies[2].wait()
    values = tokens_ref[...].astype(F32)
    scale = lax.rsqrt(jnp.mean(values * values, axis=-1, keepdims=True) + 1e-06)
    piece = width // 8
    pick = held[...].astype(BF16)
    pick_ref[...] = pick
    for s in range(2):
        at = pl.multiple_of(s * (width // 2) + q * piece, piece)
        part = tokens_ref[:, pl.ds(at, piece)].astype(F32)
        normed = (part * scale * gain_ref[:, pl.ds(at, piece)]).astype(BF16)
        sent_ref[:, s * piece : (s + 1) * piece] = jnp.dot(
            pick, normed, preferred_element_type=F32
        ).astype(BF16)


def dispatch(tokens, norm_gain, chosen, where, slots):
    experts = chosen.shape[0]
    tok_rows, width = tokens.shape
    rows = experts * slots
    vmem = pl.BlockSpec(memory_space=pltpu.VMEM)
    return pl.pallas_call(
        functools.partial(dispatch_kernel, slots),
        out_shape=(
            jax.ShapeDtypeStruct((rows, tok_rows), BF16),
            jax.ShapeDtypeStruct((rows, width // 4), BF16),
        ),
        in_specs=[pl.BlockSpec(memory_space=pltpu.SMEM)] + [pl.BlockSpec(memory_space=pltpu.HBM)] * 3,
        out_specs=(vmem, vmem),
        scratch_shapes=[
            pltpu.VMEM((rows, tok_rows), F32),
            pltpu.VMEM((tok_rows, width), BF16),
            pltpu.VMEM((1, width), F32),
            pltpu.VMEM(chosen.shape, I32),
            pltpu.SemaphoreType.DMA((3,)),
        ],
        compiler_params=pltpu.CompilerParams(vmem_limit_bytes=12 << 20),
    )(where, tokens, norm_gain.reshape(1, width), chosen)


def weight_rows(ref, j):
    return ref[:, pl.ds(j, 1), :, :].reshape(2 * ref.shape[2], ref.shape[3])


def near_kernel(y_ref, own, below_a, below_b, above_a, above_b, *refs):
    weights, totals = refs[:4], refs[4:]
    q = y_ref[0] & 3
    mid = below_a.shape[0]
    for w_ref, total in zip(weights, totals):
        w_own = weight_rows(w_ref, q)
        w_below = weight_rows(w_ref, (q + 3) & 3)
        w_above = weight_rows(w_ref, (q + 1) & 3)
        for r, (below, above) in enumerate(((below_a, above_a), (below_b, above_b))):
            rows = slice(r * mid, (r + 1) * mid)
            total[rows, :] = (
                dot(own[rows, :], w_own) + dot(below[...], w_below) + dot(above[...], w_above)
            )


def far_kernel(
    y_ref, far_a, far_b, t_gate, t_up, t_gate_m, t_up_m, gate, up, gate_m, up_m, down, down_m,
    hid, hid_m, first_a, first_b,
):
    y = y_ref[0]
    mid = far_a.shape[0]
    piece = gate.shape[2]
    w = [weight_rows(ref, (y + 2) & 3) for ref in (gate, up, gate_m, up_m)]
    at = pl.multiple_of(((y + 4) & 7) * piece, piece)
    d_own, d_mate = down[:, pl.ds(at, piece)], down_m[:, pl.ds(at, piece)]
    for r, (far, first) in enumerate(((far_a, first_a), (far_b, first_b))):
        rows = slice(r * mid, (r + 1) * mid)
        x = far[...]
        pre = [t[rows, :] + dot(x, m) for t, m in zip((t_gate, t_up, t_gate_m, t_up_m), w)]
        h_own, h_mate = [
            (pre[2 * k] / (1.0 + jnp.exp(-pre[2 * k])) * pre[2 * k + 1]).astype(BF16)
            for k in range(2)
        ]
        hid[rows, :] = h_own
        hid_m[rows, :] = h_mate
        first[...] = (dot(h_own, d_own) + dot(h_mate, d_mate)).astype(first.dtype)


def out_kernel(y_ref, hid, hid_m, down, down_m, *outs):
    y = y_ref[0]
    piece = outs[0].shape[1]
    for k, out in zip((3, -3, 2, -2, 1, -1, 0), outs):
        at = pl.multiple_of(((y + k) & 7) * piece, piece)
        out[...] = dot(hid[...], down[:, pl.ds(at, piece)]) + dot(
            hid_m[...], down_m[:, pl.ds(at, piece)]
        )


def back_kernel(y_ref, pick, own, r_up, r_down, weight, back):
    total = own[...] + r_up[...].astype(F32) + r_down[...].astype(F32)
    weighted = (total * weight[...]).astype(BF16)
    back[...] = dot(pick[...], weighted).astype(BF16)


def call_vmem(kernel, out_shape, flops, q, *arrays):
    vmem = pl.BlockSpec(memory_space=pltpu.VMEM)
    return pl.pallas_call(
        kernel,
        out_shape=out_shape,
        in_specs=[pl.BlockSpec(memory_space=pltpu.SMEM)] + [vmem] * len(arrays),
        out_specs=tuple(vmem for _ in out_shape),
        cost_estimate=pl.CostEstimate(flops=flops, bytes_accessed=8 << 20, transcendentals=0),
        compiler_params=pltpu.CompilerParams(vmem_limit_bytes=20 << 20),
    )(q, *arrays)


def shards(tokens, norm_gain, chosen, route_weight, gate_weight, up_weight, down_weight):
    tok_rows, width = tokens.shape
    experts, capacity = chosen.shape
    p = lax.axis_index("ep")
    y = lax.axis_index("y")
    c = lax.axis_index("c")
    q = lax.bitwise_and(y, 3)
    block = width // 16
    piece = 2 * block
    quarter = 2 * piece
    half_rows = capacity // 2
    mid = half_rows // 2
    slots = 3 * tok_rows // 32
    mate = [(0, 1), (1, 0)]
    up, down = shift(8, 1), shift(8, -1)

    where = jnp.stack([p * tok_rows, c, q]).astype(I32)
    pick_token, sent = dispatch(tokens, norm_gain, chosen, where, slots)
    got = lax.all_to_all(sent.reshape(experts, slots, quarter), "ep", 0, 0, tiled=True)
    got = got.reshape(experts * slots, quarter)

    gate_w, up_w, down_w, _ = lax.optimization_barrier(
        (gate_weight[0], up_weight[0], down_weight[0], sent)
    )
    gate_m = lax.ppermute(gate_w, "c", mate)
    up_m = lax.ppermute(up_w, "c", mate)
    down_m = lax.ppermute(down_w, "c", mate)

    mine = lax.dynamic_index_in_dim(chosen, p, 0, keepdims=False)
    edges = jnp.arange(experts + 1, dtype=I32) * tok_rows
    src_edge = jnp.sum((mine[None, :] < edges[:, None]).astype(I32), axis=1)
    k_edge = lax.shift_right_logical(src_edge - c + 1, 1)
    k_slot = k_edge[:-1, None] + jnp.arange(slots, dtype=I32)[None, :]
    k_slot = jnp.where(k_slot < k_edge[1:, None], k_slot, half_rows).reshape(experts * slots)
    k = jnp.arange(half_rows, dtype=I32)
    pick_row, pick_row_t = lax.optimization_barrier(
        ((k_slot[:, None] == k[None, :]).astype(BF16), (k[:, None] == k_slot[None, :]).astype(BF16))
    )
    my_weight = lax.dynamic_index_in_dim(
        route_weight.reshape(half_rows, 2), c, 1, keepdims=True
    )

    own = dot(pick_row_t, got).astype(BF16)
    own_a, own_b = own[:mid], own[mid:]
    below_a = lax.ppermute(own_a, "y", up)
    above_b = lax.ppermute(own_b, "y", down)
    below_b = lax.ppermute(own_b, "y", up)
    above_a = lax.ppermute(own_a, "y", down)
    far_a = lax.ppermute(below_a, "y", up)
    far_b = lax.ppermute(above_b, "y", down)
    def view(w):
        return w.reshape(2, 4, piece, w.shape[1])

    gates = [view(w) for w in (gate_w, up_w, gate_m, up_m)]
    units = gate_w.shape[1]
    y_one = y.astype(I32).reshape(1)
    totals = call_vmem(
        near_kernel,
        [jax.ShapeDtypeStruct((half_rows, units), F32)] * 4,
        2 * half_rows * 3 * quarter * 4 * units,
        y_one, own, below_a, below_b, above_a, above_b, *gates,
    )
    hid_shape = jax.ShapeDtypeStruct((half_rows, units), BF16)
    first_shape = jax.ShapeDtypeStruct((mid, piece), BF16)
    hid, hid_m, first_a, first_b = call_vmem(
        far_kernel,
        [hid_shape, hid_shape, first_shape, first_shape],
        2 * half_rows * (quarter * 4 * units + 2 * units * piece),
        y_one, far_a, far_b, *totals, *gates, down_w, down_m,
    )
    r_up = lax.ppermute(first_a, "y", up)
    r_down = lax.ppermute(first_b, "y", down)
    outs = call_vmem(
        out_kernel,
        [jax.ShapeDtypeStruct((half_rows, piece), F32)] * 7,
        2 * half_rows * 2 * units * 7 * piece,
        y_one, hid, hid_m, down_w, down_m,
    )
    r_up = jnp.pad(r_up, ((0, mid), (0, 0)))
    r_down = jnp.pad(r_down, ((mid, 0), (0, 0)))
    for k in range(3):
        r_up, r_down = (
            lax.ppermute((outs[2 * k] + r_up.astype(F32)).astype(BF16), "y", up),
            lax.ppermute((outs[2 * k + 1] + r_down.astype(F32)).astype(BF16), "y", down),
        )
    (back,) = call_vmem(
        back_kernel,
        [jax.ShapeDtypeStruct((experts * slots, piece), BF16)],
        2 * experts * slots * half_rows * piece,
        y_one, pick_row, outs[6], r_up, r_down, my_weight,
    )
    back = back.reshape(experts, slots, piece)
    returned = lax.all_to_all(back, "ep", 0, 0, tiled=True).reshape(experts * slots, piece)
    part = dot(pick_token, returned, OVER_ROWS)

    other = lax.dynamic_slice_in_dim(part, (1 - c) * block, block, 1).astype(BF16)
    theirs = lax.ppermute(other, "c", mate)
    combined = lax.dynamic_slice_in_dim(part, c * block, block, 1) + theirs.astype(F32)
    return combined.astype(BF16)


def solution(mesh):
    finer = Mesh(mesh.devices.reshape(mesh.shape["ep"], 8, 2), ("ep", "y", "c"))
    tp = ("y", "c")
    in_specs = (
        P("ep", None),
        P(),
        P(),
        P("ep", None),
        P("ep", None, tp),
        P("ep", None, tp),
        P("ep", tp, None),
    )
    return jax.shard_map(
        shards, mesh=finer, in_specs=in_specs, out_specs=P("ep", tp), check_vma=False
    )
```

```python
import functools

import jax
import jax.numpy as jnp
from jax import lax
from jax.experimental import pallas as pl
from jax.experimental.pallas import tpu as pltpu
from jax.sharding import Mesh
from jax.sharding import PartitionSpec as P


BF16 = jnp.bfloat16
F32 = jnp.float32
I32 = jnp.int32
OVER_ROWS = (((0,), (0,)), ((), ()))


def shift(n, k):
    return [(i, (i + k) % n) for i in range(n)]


def dot(a, b, dims=(((1,), (0,)), ((), ()))):
    return lax.dot_general(a, b, dims, preferred_element_type=F32)


def dispatch_kernel(
    slots, where_ref, tokens_in, gain_in, chosen_in, pick_ref, sent_ref,
    held, tokens_ref, gain_ref, chosen_ref, sems,
):
    copies = [
        pltpu.make_async_copy(chosen_in, chosen_ref, sems.at[0]),
        pltpu.make_async_copy(tokens_in, tokens_ref, sems.at[1]),
        pltpu.make_async_copy(gain_in, gain_ref, sems.at[2]),
    ]
    for copy in copies:
        copy.start()
    copies[0].wait()
    tok_rows, width = tokens_ref.shape
    experts, capacity = chosen_ref.shape
    first_token, parity, q = where_ref[0], where_ref[1], where_ref[2]
    chosen = chosen_ref[...]
    run_start = jnp.sum((chosen < first_token).astype(I32), axis=1, keepdims=True)
    run_end = jnp.sum((chosen < first_token + tok_rows).astype(I32), axis=1, keepdims=True)
    first = run_start + ((run_start + parity) & 1)
    rank = lax.broadcasted_iota(I32, (slots, capacity), 1)
    step = 2 * lax.broadcasted_iota(I32, (slots, capacity), 0)
    ahead = rank - step
    slot = 2 * lax.broadcasted_iota(I32, (slots, 1), 0)
    column = lax.broadcasted_iota(I32, (slots, tok_rows), 1)
    for e in range(experts):
        start = first[e : e + 1, :]
        token = jnp.sum(
            jnp.where(ahead == start, chosen[e : e + 1, :], 0), axis=1, keepdims=True
        )
        local = jnp.where(slot + start < run_end[e : e + 1, :], token - first_token, tok_rows)
        held[e * slots : (e + 1) * slots, :] = (column == local).astype(F32)
    copies[1].wait()
    copies[2].wait()
    values = tokens_ref[...].astype(F32)
    scale = lax.rsqrt(jnp.mean(values * values, axis=-1, keepdims=True) + 1e-06)
    piece = width // 8
    pick = held[...].astype(BF16)
    pick_ref[...] = pick
    for s in range(2):
        at = pl.multiple_of(s * (width // 2) + q * piece, piece)
        part = tokens_ref[:, pl.ds(at, piece)].astype(F32)
        normed = (part * scale * gain_ref[:, pl.ds(at, piece)]).astype(BF16)
        sent_ref[:, s * piece : (s + 1) * piece] = jnp.dot(
            pick, normed, preferred_element_type=F32
        ).astype(BF16)


def dispatch(tokens, norm_gain, chosen, where, slots):
    experts = chosen.shape[0]
    tok_rows, width = tokens.shape
    rows = experts * slots
    vmem = pl.BlockSpec(memory_space=pltpu.VMEM)
    return pl.pallas_call(
        functools.partial(dispatch_kernel, slots),
        out_shape=(
            jax.ShapeDtypeStruct((rows, tok_rows), BF16),
            jax.ShapeDtypeStruct((rows, width // 4), BF16),
        ),
        in_specs=[pl.BlockSpec(memory_space=pltpu.SMEM)] + [pl.BlockSpec(memory_space=pltpu.HBM)] * 3,
        out_specs=(vmem, vmem),
        scratch_shapes=[
            pltpu.VMEM((rows, tok_rows), F32),
            pltpu.VMEM((tok_rows, width), BF16),
            pltpu.VMEM((1, width), F32),
            pltpu.VMEM(chosen.shape, I32),
            pltpu.SemaphoreType.DMA((3,)),
        ],
        compiler_params=pltpu.CompilerParams(vmem_limit_bytes=60 << 20),
    )(where, tokens, norm_gain.reshape(1, width), chosen)


def weight_rows(ref, j):
    return ref[:, pl.ds(j, 1), :, :].reshape(2 * ref.shape[2], ref.shape[3])


def flat(rows):
    return rows.reshape(rows.shape[0] * rows.shape[1], rows.shape[2])


def columns(ref, y, k, piece):
    return ref.at[:, pl.ds(pl.multiple_of(((y + k) & 7) * piece, piece), piece)]


def near_kernel(y_ref, own, below_a, below_b, above_a, above_b, gate, up, gate_m, up_m, *refs):
    totals, held, sems = refs[:4], refs[4], refs[5]
    q = y_ref[0] & 3
    quarters = (q, (q + 3) & 3, (q + 1) & 3)
    mid = below_a.shape[0]
    copies = [
        [pltpu.make_async_copy(m.at[:, j], held.at[n, i], sems.at[n, i]) for i, j in enumerate(quarters)]
        for n, m in enumerate((gate_m, up_m))
    ]
    for row in copies:
        for copy in row:
            copy.start()
    for n, total in enumerate(totals):
        if n < 2:
            w_own, w_below, w_above = [weight_rows((gate, up)[n], j) for j in quarters]
        else:
            for copy in copies[n - 2]:
                copy.wait()
            w_own, w_below, w_above = [flat(held[n - 2, i]) for i in range(3)]
        for r, (below, above) in enumerate(((below_a, above_a), (below_b, above_b))):
            rows = slice(r * mid, (r + 1) * mid)
            total[rows, :] = (
                dot(own[rows, :], w_own) + dot(below[...], w_below) + dot(above[...], w_above)
            )


def far_kernel(
    y_ref, far_a, far_b, t_gate, t_up, t_gate_m, t_up_m, gate, up, down, gate_m, up_m, down_m,
    hid, hid_m, first_a, first_b, held, held_down, sems,
):
    y = y_ref[0]
    j_far = (y + 2) & 3
    mid = far_a.shape[0]
    piece = first_a.shape[1]
    copies = [
        pltpu.make_async_copy(gate_m.at[:, j_far], held.at[0], sems.at[0]),
        pltpu.make_async_copy(up_m.at[:, j_far], held.at[1], sems.at[1]),
        pltpu.make_async_copy(columns(down_m, y, 4, piece), held_down, sems.at[2]),
    ]
    for copy in copies:
        copy.start()
    d_own = columns(down, y, 4, piece)[...]
    halves = ((slice(0, mid), far_a, first_a), (slice(mid, 2 * mid), far_b, first_b))

    def gated(rows, x, t_g, t_u, w_g, w_u):
        g = t_g[rows, :] + dot(x, w_g)
        u = t_u[rows, :] + dot(x, w_u)
        return (g / (1.0 + jnp.exp(-g)) * u).astype(BF16)

    w_gate, w_up = weight_rows(gate, j_far), weight_rows(up, j_far)
    partial = []
    for rows, far, _ in halves:
        h_own = gated(rows, far[...], t_gate, t_up, w_gate, w_up)
        hid[rows, :] = h_own
        partial.append(dot(h_own, d_own))
    for copy in copies:
        copy.wait()
    w_gate, w_up = flat(held[0]), flat(held[1])
    for (rows, far, first), part in zip(halves, partial):
        h_mate = gated(rows, far[...], t_gate_m, t_up_m, w_gate, w_up)
        hid_m[rows, :] = h_mate
        first[...] = (part + dot(h_mate, held_down[...])).astype(first.dtype)


def out_kernel(offsets, y_ref, hid, hid_m, down, down_m, *refs):
    outs, held, sems = refs[:-2], refs[-2], refs[-1]
    y = y_ref[0]
    piece = outs[0].shape[1]
    copies = [
        pltpu.make_async_copy(columns(down_m, y, k, piece), held.at[n], sems.at[n])
        for n, k in enumerate(offsets)
    ]
    for copy in copies:
        copy.start()
    for n, (k, out) in enumerate(zip(offsets, outs)):
        value = dot(hid[...], columns(down, y, k, piece)[...])
        copies[n].wait()
        out[...] = (value + dot(hid_m[...], held[n])).astype(out.dtype)


def back_kernel(y_ref, pick, own, r_up, r_down, weight, back):
    total = own[...] + r_up[...].astype(F32) + r_down[...].astype(F32)
    weighted = (total * weight[...]).astype(BF16)
    back[...] = dot(pick[...], weighted).astype(BF16)


def call_vmem(kernel, out_shape, flops, y, arrays, apart=(), scratch=()):
    vmem = pl.BlockSpec(memory_space=pltpu.VMEM)
    return pl.pallas_call(
        kernel,
        out_shape=out_shape,
        in_specs=[pl.BlockSpec(memory_space=pltpu.SMEM)]
        + [vmem] * len(arrays)
        + [pl.BlockSpec(memory_space=pl.ANY)] * len(apart),
        out_specs=tuple(vmem for _ in out_shape),
        scratch_shapes=list(scratch),
        cost_estimate=pl.CostEstimate(flops=flops, bytes_accessed=8 << 20, transcendentals=0),
        compiler_params=pltpu.CompilerParams(vmem_limit_bytes=20 << 20),
    )(y, *arrays, *apart)


def shards(tokens, norm_gain, chosen, route_weight, gate_weight, up_weight, down_weight):
    tok_rows, width = tokens.shape
    experts, capacity = chosen.shape
    p = lax.axis_index("ep")
    y = lax.axis_index("y")
    c = lax.axis_index("c")
    q = lax.bitwise_and(y, 3)
    block = width // 16
    piece = 2 * block
    quarter = 2 * piece
    half_rows = capacity // 2
    mid = half_rows // 2
    slots = 3 * tok_rows // 32
    mate = [(0, 1), (1, 0)]
    up, down = shift(8, 1), shift(8, -1)

    where = jnp.stack([p * tok_rows, c, q]).astype(I32)
    pick_token, sent = dispatch(tokens, norm_gain, chosen, where, slots)
    got = lax.all_to_all(sent.reshape(experts, slots, quarter), "ep", 0, 0, tiled=True)
    got = got.reshape(experts * slots, quarter)

    gate_w, up_w, down_w, _ = lax.optimization_barrier(
        (gate_weight[0], up_weight[0], down_weight[0], sent)
    )
    gate_m = lax.ppermute(gate_w, "c", mate)
    up_m = lax.ppermute(up_w, "c", mate)
    down_m = lax.ppermute(down_w, "c", mate)

    mine = lax.dynamic_index_in_dim(chosen, p, 0, keepdims=False)
    edges = jnp.arange(experts + 1, dtype=I32) * tok_rows
    src_edge = jnp.sum((mine[None, :] < edges[:, None]).astype(I32), axis=1)
    k_edge = lax.shift_right_logical(src_edge - c + 1, 1)
    k_slot = k_edge[:-1, None] + jnp.arange(slots, dtype=I32)[None, :]
    k_slot = jnp.where(k_slot < k_edge[1:, None], k_slot, half_rows).reshape(experts * slots)
    k = jnp.arange(half_rows, dtype=I32)
    pick_row, pick_row_t = lax.optimization_barrier(
        ((k_slot[:, None] == k[None, :]).astype(BF16), (k[:, None] == k_slot[None, :]).astype(BF16))
    )
    my_weight = lax.dynamic_index_in_dim(
        route_weight.reshape(half_rows, 2), c, 1, keepdims=True
    )

    own = dot(pick_row_t, got).astype(BF16)
    own_a, own_b = own[:mid], own[mid:]
    below_a = lax.ppermute(own_a, "y", up)
    above_b = lax.ppermute(own_b, "y", down)
    below_b = lax.ppermute(own_b, "y", up)
    above_a = lax.ppermute(own_a, "y", down)
    far_a = lax.ppermute(below_a, "y", up)
    far_b = lax.ppermute(above_b, "y", down)

    def view(w):
        return w.reshape(2, 4, piece, w.shape[1])

    gates, gates_m = [view(gate_w), view(up_w)], [view(gate_m), view(up_m)]
    units = gate_w.shape[1]
    y_one = y.astype(I32).reshape(1)
    weight_piece = (2, piece, units)
    totals = call_vmem(
        near_kernel,
        [jax.ShapeDtypeStruct((half_rows, units), F32)] * 4,
        2 * half_rows * 3 * quarter * 4 * units,
        y_one,
        [own, below_a, below_b, above_a, above_b, *gates],
        gates_m,
        [pltpu.VMEM((2, 3) + weight_piece, BF16), pltpu.SemaphoreType.DMA((2, 3))],
    )
    hid_shape = jax.ShapeDtypeStruct((half_rows, units), BF16)
    first_shape = jax.ShapeDtypeStruct((mid, piece), BF16)
    hid, hid_m, first_a, first_b = call_vmem(
        far_kernel,
        [hid_shape, hid_shape, first_shape, first_shape],
        2 * half_rows * (quarter * 4 * units + 2 * units * piece),
        y_one,
        [far_a, far_b, *totals, *gates, down_w],
        [*gates_m, down_m],
        [
            pltpu.VMEM((2,) + weight_piece, BF16),
            pltpu.VMEM((units, piece), BF16),
            pltpu.SemaphoreType.DMA((3,)),
        ],
    )

    def outs_at(offsets, dtype):
        return call_vmem(
            functools.partial(out_kernel, offsets),
            [jax.ShapeDtypeStruct((half_rows, piece), dtype)] * len(offsets),
            2 * half_rows * 2 * units * len(offsets) * piece,
            y_one,
            [hid, hid_m, down_w],
            [down_m],
            [
                pltpu.VMEM((len(offsets), units, piece), BF16),
                pltpu.SemaphoreType.DMA((len(offsets),)),
            ],
        )

    jump_up = lax.ppermute(first_a, "y", shift(8, 2))
    jump_down = lax.ppermute(first_b, "y", shift(8, -2))
    up_3, down_3 = outs_at((3, -3), BF16)
    r_up = lax.ppermute(up_3, "y", up)
    r_down = lax.ppermute(down_3, "y", down)
    up_2, down_2, up_1, down_1, own_out = outs_at((2, -2, 1, -1, 0), F32)
    up_2 = up_2 + jnp.pad(jump_up.astype(F32), ((0, mid), (0, 0)))
    down_2 = down_2 + jnp.pad(jump_down.astype(F32), ((mid, 0), (0, 0)))
    for mine_up, mine_down in ((up_2, down_2), (up_1, down_1)):
        r_up, r_down = (
            lax.ppermute((mine_up + r_up.astype(F32)).astype(BF16), "y", up),
            lax.ppermute((mine_down + r_down.astype(F32)).astype(BF16), "y", down),
        )
    (back,) = call_vmem(
        back_kernel,
        [jax.ShapeDtypeStruct((experts * slots, piece), BF16)],
        2 * experts * slots * half_rows * piece,
        y_one,
        [pick_row, own_out, r_up, r_down, my_weight],
    )
    back = back.reshape(experts, slots, piece)
    returned = lax.all_to_all(back, "ep", 0, 0, tiled=True).reshape(experts * slots, piece)
    part = dot(pick_token, returned, OVER_ROWS)

    other = lax.dynamic_slice_in_dim(part, (1 - c) * block, block, 1).astype(BF16)
    theirs = lax.ppermute(other, "c", mate)
    combined = lax.dynamic_slice_in_dim(part, c * block, block, 1) + theirs.astype(F32)
    return combined.astype(BF16)


def solution(mesh):
    finer = Mesh(mesh.devices.reshape(mesh.shape["ep"], 8, 2), ("ep", "y", "c"))
    tp = ("y", "c")
    in_specs = (
        P("ep", None),
        P(),
        P(),
        P("ep", None),
        P("ep", None, tp),
        P("ep", None, tp),
        P("ep", tp, None),
    )

    return jax.shard_map(
        shards, mesh=finer, in_specs=in_specs, out_specs=P("ep", tp), check_vma=False
    )
```

```python
import functools

import jax
import jax.numpy as jnp
from jax import lax
from jax.experimental import pallas as pl
from jax.experimental.pallas import tpu as pltpu
from jax.sharding import Mesh
from jax.sharding import PartitionSpec as P


BF16 = jnp.bfloat16
F32 = jnp.float32
I32 = jnp.int32
OVER_ROWS = (((0,), (0,)), ((), ()))


def dot(a, b, dims=(((1,), (0,)), ((), ()))):
    return lax.dot_general(a, b, dims, preferred_element_type=F32)


def dispatch_kernel(
    slots, where_ref, tokens_in, gain_in, chosen_in, pick_ref, sent_ref,
    held, tokens_ref, gain_ref, chosen_ref, sems,
):
    copies = [
        pltpu.make_async_copy(chosen_in, chosen_ref, sems.at[0]),
        pltpu.make_async_copy(tokens_in, tokens_ref, sems.at[1]),
        pltpu.make_async_copy(gain_in, gain_ref, sems.at[2]),
    ]
    for copy in copies:
        copy.start()
    copies[0].wait()
    tok_rows, width = tokens_ref.shape
    experts, capacity = chosen_ref.shape
    q, first_token, parity = where_ref[0] & 3, where_ref[2], where_ref[3]
    chosen = chosen_ref[...]
    run_start = jnp.sum((chosen < first_token).astype(I32), axis=1, keepdims=True)
    run_end = jnp.sum((chosen < first_token + tok_rows).astype(I32), axis=1, keepdims=True)
    first = run_start + ((run_start + parity) & 1)
    rank = lax.broadcasted_iota(I32, (slots, capacity), 1)
    step = 2 * lax.broadcasted_iota(I32, (slots, capacity), 0)
    ahead = rank - step
    slot = 2 * lax.broadcasted_iota(I32, (slots, 1), 0)
    column = lax.broadcasted_iota(I32, (slots, tok_rows), 1)
    for e in range(experts):
        start = first[e : e + 1, :]
        token = jnp.sum(
            jnp.where(ahead == start, chosen[e : e + 1, :], 0), axis=1, keepdims=True
        )
        local = jnp.where(slot + start < run_end[e : e + 1, :], token - first_token, tok_rows)
        held[e * slots : (e + 1) * slots, :] = (column == local).astype(F32)
    copies[1].wait()
    copies[2].wait()
    values = tokens_ref[...].astype(F32)
    scale = lax.rsqrt(jnp.mean(values * values, axis=-1, keepdims=True) + 1e-06)
    piece = width // 8
    pick = held[...].astype(BF16)
    pick_ref[...] = pick
    for s in range(2):
        at = pl.multiple_of(s * (width // 2) + q * piece, piece)
        part = tokens_ref[:, pl.ds(at, piece)].astype(F32)
        normed = (part * scale * gain_ref[:, pl.ds(at, piece)]).astype(BF16)
        sent_ref[:, s * piece : (s + 1) * piece] = jnp.dot(
            pick, normed, preferred_element_type=F32
        ).astype(BF16)


def dispatch(tokens, norm_gain, chosen, where, slots):
    experts = chosen.shape[0]
    tok_rows, width = tokens.shape
    rows = experts * slots
    vmem = pl.BlockSpec(memory_space=pltpu.VMEM)
    return pl.pallas_call(
        functools.partial(dispatch_kernel, slots),
        out_shape=(
            jax.ShapeDtypeStruct((rows, tok_rows), BF16),
            jax.ShapeDtypeStruct((rows, width // 4), BF16),
        ),
        in_specs=[pl.BlockSpec(memory_space=pltpu.SMEM)] + [pl.BlockSpec(memory_space=pltpu.HBM)] * 3,
        out_specs=(vmem, vmem),
        scratch_shapes=[
            pltpu.VMEM((rows, tok_rows), F32),
            pltpu.VMEM((tok_rows, width), BF16),
            pltpu.VMEM((1, width), F32),
            pltpu.VMEM(chosen.shape, I32),
            pltpu.SemaphoreType.DMA((3,)),
        ],
        compiler_params=pltpu.CompilerParams(vmem_limit_bytes=60 << 20),
    )(where, tokens, norm_gain.reshape(1, width), chosen)


def flat(rows):
    return rows.reshape(rows.shape[0] * rows.shape[1], rows.shape[2])


def columns(ref, where_ref, k, piece):
    j = (where_ref[0] + k * where_ref[1]) & 7
    return ref[:, pl.ds(pl.multiple_of(j * piece, piece), piece)]


def near_kernel(where_ref, own, major, minor, *refs):
    weights, totals, far_rows, held, sems = refs[:4], refs[4:8], refs[8], refs[9], refs[10]
    y, d = where_ref[0], where_ref[1]
    quarters = (y & 3, (y - d) & 3, (y + d) & 3, (y + 2) & 3)
    copies = [
        [
            pltpu.make_async_copy(
                w.at[:, j], held.at[n, i] if i < 3 else far_rows.at[n], sems.at[n, i]
            )
            for i, j in enumerate(quarters)
        ]
        for n, w in enumerate(weights)
    ]
    for i in range(4):
        for n in range(4):
            copies[n][i].start()
    for n, total in enumerate(totals):
        for copy in copies[n][:3]:
            copy.wait()
        total[...] = (
            dot(own[...], flat(held[n, 0]))
            + dot(major[...], flat(held[n, 1]))
            + dot(minor[...], flat(held[n, 2]))
        )
    for n in range(4):
        copies[n][3].wait()


def far_kernel(where_ref, far, t_gate, t_up, t_gate_m, t_up_m, far_rows, down, down_m, hid, hid_m, first):
    piece = first.shape[1]
    d_own = columns(down, where_ref, 4, piece)
    d_mate = columns(down_m, where_ref, 4, piece)
    mid = far.shape[0] // 2

    def gated(rows, t_g, t_u, w_g, w_u):
        g = t_g[rows, :] + dot(far[rows, :], w_g)
        u = t_u[rows, :] + dot(far[rows, :], w_u)
        return (g / (1.0 + jnp.exp(-g)) * u).astype(BF16)

    w = [flat(far_rows[n]) for n in range(4)]
    for r in range(2):
        rows = slice(r * mid, (r + 1) * mid)
        h_own = gated(rows, t_gate, t_up, w[0], w[1])
        h_mate = gated(rows, t_gate_m, t_up_m, w[2], w[3])
        hid[rows, :] = h_own
        hid_m[rows, :] = h_mate
        first[rows, :] = (dot(h_own, d_own) + dot(h_mate, d_mate)).astype(first.dtype)


def out_kernel(offsets, where_ref, hid, hid_m, down, down_m, *outs):
    piece = outs[0].shape[1]
    for k, out in zip(offsets, outs):
        value = dot(hid[...], columns(down, where_ref, k, piece))
        value = value + dot(hid_m[...], columns(down_m, where_ref, k, piece))
        out[...] = value.astype(out.dtype)


def own_kernel(where_ref, k_slot, got, own):
    row = lax.broadcasted_iota(I32, (own.shape[0], got.shape[0]), 0)
    pick = (row == k_slot[...]).astype(F32).astype(BF16)
    own[...] = dot(pick, got[...]).astype(BF16)


def back_kernel(where_ref, k_slot, own, r_major, r_minor, weight, back):
    row = lax.broadcasted_iota(I32, (back.shape[0], own.shape[0]), 1)
    pick = (row == k_slot[...]).astype(F32).astype(BF16)
    total = own[...] + r_major[...].astype(F32) + r_minor[...].astype(F32)
    weighted = (total * weight[...]).astype(BF16)
    back[...] = dot(pick, weighted).astype(BF16)


def call_vmem(kernel, out_shape, flops, where, arrays, apart=(), scratch=()):
    vmem = pl.BlockSpec(memory_space=pltpu.VMEM)
    return pl.pallas_call(
        kernel,
        out_shape=out_shape,
        in_specs=[pl.BlockSpec(memory_space=pltpu.SMEM)]
        + [vmem] * len(arrays)
        + [pl.BlockSpec(memory_space=pl.ANY)] * len(apart),
        out_specs=tuple(vmem for _ in out_shape),
        scratch_shapes=list(scratch),
        cost_estimate=pl.CostEstimate(flops=flops, bytes_accessed=8 << 20, transcendentals=0),
        compiler_params=pltpu.CompilerParams(vmem_limit_bytes=20 << 20),
    )(where, *arrays, *apart)


def shards(tokens, norm_gain, chosen, route_weight, gate_weight, up_weight, down_weight):
    tok_rows, width = tokens.shape
    experts, capacity = chosen.shape
    p = lax.axis_index("ep")
    y = lax.axis_index("y")
    c = lax.axis_index("c")
    block = width // 16
    piece = 2 * block
    quarter = 2 * piece
    half_rows = capacity // 2
    slots = 3 * tok_rows // 32
    mate = [(0, 1), (1, 0)]
    tp = ("y", "c")
    to_major = [(2 * i + j, 2 * ((i + 1 - 2 * j) % 8) + j) for i in range(8) for j in range(2)]
    to_minor = [(target, source) for source, target in to_major]

    place = jnp.stack([y, 1 - 2 * c, p * tok_rows, c]).astype(I32)
    pick_token, sent = dispatch(tokens, norm_gain, chosen, place, slots)
    got = lax.all_to_all(sent.reshape(experts, slots, quarter), "ep", 0, 0, tiled=True)
    got = got.reshape(experts * slots, quarter)

    gate_w, up_w, down_w, _ = lax.optimization_barrier(
        (gate_weight[0], up_weight[0], down_weight[0], sent)
    )
    gate_m = lax.ppermute(gate_w, "c", mate)
    up_m = lax.ppermute(up_w, "c", mate)
    down_m = lax.ppermute(down_w, "c", mate)

    mine = lax.dynamic_index_in_dim(chosen, p, 0, keepdims=False)
    edges = jnp.arange(experts + 1, dtype=I32) * tok_rows
    src_edge = jnp.sum((mine[None, :] < edges[:, None]).astype(I32), axis=1)
    k_edge = lax.shift_right_logical(src_edge - c + 1, 1)
    k_slot = k_edge[:-1, None] + jnp.arange(slots, dtype=I32)[None, :]
    k_slot = jnp.where(k_slot < k_edge[1:, None], k_slot, half_rows).reshape(experts * slots)
    my_weight = lax.dynamic_index_in_dim(
        route_weight.reshape(half_rows, 2), c, 1, keepdims=True
    )

    (own,) = call_vmem(
        own_kernel,
        [jax.ShapeDtypeStruct((half_rows, quarter), BF16)],
        2 * half_rows * experts * slots * quarter,
        place,
        [k_slot.reshape(1, experts * slots), got],
    )
    major = lax.ppermute(own, tp, to_major)
    minor = lax.ppermute(own, tp, to_minor)
    far = lax.ppermute(major, tp, to_major)

    def view(w):
        return w.reshape(2, 4, piece, w.shape[1])

    units = gate_w.shape[1]
    *totals, far_rows = call_vmem(
        near_kernel,
        [jax.ShapeDtypeStruct((half_rows, units), F32)] * 4
        + [jax.ShapeDtypeStruct((4, 2, piece, units), BF16)],
        2 * half_rows * 3 * quarter * 4 * units,
        place,
        [own, major, minor],
        [view(w) for w in (gate_w, up_w, gate_m, up_m)],
        [pltpu.VMEM((4, 3, 2, piece, units), BF16), pltpu.SemaphoreType.DMA((4, 4))],
    )
    hid_shape = jax.ShapeDtypeStruct((half_rows, units), BF16)
    hid, hid_m, first = call_vmem(
        far_kernel,
        [hid_shape, hid_shape, jax.ShapeDtypeStruct((half_rows, piece), BF16)],
        2 * half_rows * (quarter * 4 * units + 2 * units * piece),
        place,
        [far, *totals, far_rows, down_w, down_m],
    )

    def outs_at(offsets, dtype):
        return call_vmem(
            functools.partial(out_kernel, offsets),
            [jax.ShapeDtypeStruct((half_rows, piece), dtype)] * len(offsets),
            2 * half_rows * 2 * units * len(offsets) * piece,
            place,
            [hid, hid_m, down_w, down_m],
        )

    def passed(mine, received):
        return (mine + received.astype(F32)).astype(BF16)

    r_major = lax.ppermute(first, tp, to_major)
    near_3, far_3 = outs_at((-3, 3), F32)
    r_minor = lax.ppermute(near_3.astype(BF16), tp, to_minor)
    r_major = lax.ppermute(passed(far_3, r_major), tp, to_major)
    near_2, far_2 = outs_at((-2, 2), F32)
    r_minor = lax.ppermute(passed(near_2, r_minor), tp, to_minor)
    r_major = lax.ppermute(passed(far_2, r_major), tp, to_major)
    near_1, far_1, own_out = outs_at((-1, 1, 0), F32)
    r_minor = lax.ppermute(passed(near_1, r_minor), tp, to_minor)
    r_major = lax.ppermute(passed(far_1, r_major), tp, to_major)
    (back,) = call_vmem(
        back_kernel,
        [jax.ShapeDtypeStruct((experts * slots, piece), BF16)],
        2 * experts * slots * half_rows * piece,
        place,
        [k_slot.reshape(experts * slots, 1), own_out, r_major, r_minor, my_weight],
    )
    back = back.reshape(experts, slots, piece)
    returned = lax.all_to_all(back, "ep", 0, 0, tiled=True).reshape(experts * slots, piece)
    part = dot(pick_token, returned, OVER_ROWS)

    other = lax.dynamic_slice_in_dim(part, (1 - c) * block, block, 1).astype(BF16)
    theirs = lax.ppermute(other, "c", mate)
    combined = lax.dynamic_slice_in_dim(part, c * block, block, 1) + theirs.astype(F32)
    return combined.astype(BF16)


def solution(mesh):
    finer = Mesh(mesh.devices.reshape(mesh.shape["ep"], 8, 2), ("ep", "y", "c"))
    tp = ("y", "c")
    in_specs = (
        P("ep", None),
        P(),
        P(),
        P("ep", None),
        P("ep", None, tp),
        P("ep", None, tp),
        P("ep", tp, None),
    )

    return jax.shard_map(
        shards, mesh=finer, in_specs=in_specs, out_specs=P("ep", tp), check_vma=False
    )
```

```python
import functools

import jax
import jax.numpy as jnp
from jax import lax
from jax.experimental import pallas as pl
from jax.experimental.pallas import tpu as pltpu
from jax.sharding import Mesh
from jax.sharding import PartitionSpec as P


BF16 = jnp.bfloat16
F32 = jnp.float32
I32 = jnp.int32
OVER_ROWS = (((0,), (0,)), ((), ()))


def dot(a, b, dims=(((1,), (0,)), ((), ()))):
    return lax.dot_general(a, b, dims, preferred_element_type=F32)


def dispatch_kernel(
    slots, where_ref, tokens_in, gain_in, chosen_in, pick_ref, sent_ref,
    held, tokens_ref, gain_ref, chosen_ref, sems,
):
    copies = [
        pltpu.make_async_copy(chosen_in, chosen_ref, sems.at[0]),
        pltpu.make_async_copy(tokens_in, tokens_ref, sems.at[1]),
        pltpu.make_async_copy(gain_in, gain_ref, sems.at[2]),
    ]
    for copy in copies:
        copy.start()
    copies[0].wait()
    tok_rows, width = tokens_ref.shape
    experts, capacity = chosen_ref.shape
    q, first_token, parity = where_ref[0] & 3, where_ref[2], where_ref[3]
    chosen = chosen_ref[...]
    run_start = jnp.sum((chosen < first_token).astype(I32), axis=1, keepdims=True)
    run_end = jnp.sum((chosen < first_token + tok_rows).astype(I32), axis=1, keepdims=True)
    first = run_start + ((run_start + parity) & 1)
    rank = lax.broadcasted_iota(I32, (slots, capacity), 1)
    step = 2 * lax.broadcasted_iota(I32, (slots, capacity), 0)
    ahead = rank - step
    slot = 2 * lax.broadcasted_iota(I32, (slots, 1), 0)
    column = lax.broadcasted_iota(I32, (slots, tok_rows), 1)
    for e in range(experts):
        start = first[e : e + 1, :]
        token = jnp.sum(
            jnp.where(ahead == start, chosen[e : e + 1, :], 0), axis=1, keepdims=True
        )
        local = jnp.where(slot + start < run_end[e : e + 1, :], token - first_token, tok_rows)
        held[e * slots : (e + 1) * slots, :] = (column == local).astype(F32)
    copies[1].wait()
    copies[2].wait()
    values = tokens_ref[...].astype(F32)
    scale = lax.rsqrt(jnp.mean(values * values, axis=-1, keepdims=True) + 1e-06)
    piece = width // 8
    pick = held[...].astype(BF16)
    pick_ref[...] = pick
    for s in range(2):
        at = pl.multiple_of(s * (width // 2) + q * piece, piece)
        part = tokens_ref[:, pl.ds(at, piece)].astype(F32)
        normed = (part * scale * gain_ref[:, pl.ds(at, piece)]).astype(BF16)
        sent_ref[:, s * piece : (s + 1) * piece] = jnp.dot(
            pick, normed, preferred_element_type=F32
        ).astype(BF16)


def dispatch(tokens, norm_gain, chosen, where, slots):
    experts = chosen.shape[0]
    tok_rows, width = tokens.shape
    rows = experts * slots
    vmem = pl.BlockSpec(memory_space=pltpu.VMEM)
    return pl.pallas_call(
        functools.partial(dispatch_kernel, slots),
        out_shape=(
            jax.ShapeDtypeStruct((rows, tok_rows), BF16),
            jax.ShapeDtypeStruct((rows, width // 4), BF16),
        ),
        in_specs=[pl.BlockSpec(memory_space=pltpu.SMEM)] + [pl.BlockSpec(memory_space=pltpu.HBM)] * 3,
        out_specs=(vmem, vmem),
        scratch_shapes=[
            pltpu.VMEM((rows, tok_rows), F32),
            pltpu.VMEM((tok_rows, width), BF16),
            pltpu.VMEM((1, width), F32),
            pltpu.VMEM(chosen.shape, I32),
            pltpu.SemaphoreType.DMA((3,)),
        ],
        compiler_params=pltpu.CompilerParams(vmem_limit_bytes=60 << 20),
    )(where, tokens, norm_gain.reshape(1, width), chosen)


def flat(rows):
    return rows.reshape(rows.shape[0] * rows.shape[1], rows.shape[2])


def columns(ref, where_ref, k, piece):
    j = (where_ref[0] + k * where_ref[1]) & 7
    return ref[:, pl.ds(pl.multiple_of(j * piece, piece), piece)]


def near_kernel(where_ref, own, major_a, major_b, minor_a, minor_b, *refs):
    weights, totals, far_rows, held, sems = refs[:4], refs[4:8], refs[8], refs[9], refs[10]
    y, d = where_ref[0], where_ref[1]
    quarters = (y & 3, (y - d) & 3, (y + d) & 3, (y + 2) & 3)
    copies = [
        [
            pltpu.make_async_copy(
                w.at[:, j], held.at[n, i] if i < 3 else far_rows.at[n], sems.at[n, i]
            )
            for i, j in enumerate(quarters)
        ]
        for n, w in enumerate(weights)
    ]
    for row in copies:
        for copy in row[:3]:
            copy.start()
    for row in copies:
        row[3].start()
    mid = major_a.shape[0]
    for n, total in enumerate(totals):
        for copy in copies[n][:3]:
            copy.wait()
        w_own, w_major, w_minor = [flat(held[n, i]) for i in range(3)]
        for r, (major, minor) in enumerate(((major_a, minor_a), (major_b, minor_b))):
            rows = slice(r * mid, (r + 1) * mid)
            total[rows, :] = (
                dot(own[rows, :], w_own) + dot(major[...], w_major) + dot(minor[...], w_minor)
            )
    for row in copies:
        row[3].wait()


def far_kernel(
    where_ref, far_a, far_b, t_gate, t_up, t_gate_m, t_up_m, far_rows, down, down_m,
    hid, hid_m, first_a, first_b,
):
    mid, piece = first_a.shape
    d_own = columns(down, where_ref, 4, piece)
    d_mate = columns(down_m, where_ref, 4, piece)
    w = [flat(far_rows[n]) for n in range(4)]
    for r, (far, first) in enumerate(((far_a, first_a), (far_b, first_b))):
        rows = slice(r * mid, (r + 1) * mid)

        def gated(t_g, t_u, w_g, w_u):
            g = t_g[rows, :] + dot(far[...], w_g)
            u = t_u[rows, :] + dot(far[...], w_u)
            return (g / (1.0 + jnp.exp(-g)) * u).astype(BF16)

        h_own = gated(t_gate, t_up, w[0], w[1])
        h_mate = gated(t_gate_m, t_up_m, w[2], w[3])
        hid[rows, :] = h_own
        hid_m[rows, :] = h_mate
        first[...] = (dot(h_own, d_own) + dot(h_mate, d_mate)).astype(first.dtype)


def out_kernel(offsets, where_ref, hid, hid_m, down, down_m, *outs):
    piece = outs[0].shape[1]
    for k, out in zip(offsets, outs):
        value = dot(hid[...], columns(down, where_ref, k, piece))
        value = value + dot(hid_m[...], columns(down_m, where_ref, k, piece))
        out[...] = value.astype(out.dtype)


def own_kernel(where_ref, k_slot, got, own, own_a, own_b):
    row = lax.broadcasted_iota(I32, (own.shape[0], got.shape[0]), 0)
    pick = (row == k_slot[...]).astype(F32).astype(BF16)
    rows = dot(pick, got[...]).astype(BF16)
    mid = own_a.shape[0]
    own[...] = rows
    own_a[...] = rows[:mid, :]
    own_b[...] = rows[mid:, :]


def back_kernel(where_ref, k_slot, own, r_major, r_minor, weight, back):
    row = lax.broadcasted_iota(I32, (back.shape[0], own.shape[0]), 1)
    pick = (row == k_slot[...]).astype(F32).astype(BF16)
    total = own[...] + r_major[...].astype(F32) + r_minor[...].astype(F32)
    weighted = (total * weight[...]).astype(BF16)
    back[...] = dot(pick, weighted).astype(BF16)


def call_vmem(kernel, out_shape, flops, where, arrays, apart=(), scratch=()):
    vmem = pl.BlockSpec(memory_space=pltpu.VMEM)
    return pl.pallas_call(
        kernel,
        out_shape=out_shape,
        in_specs=[pl.BlockSpec(memory_space=pltpu.SMEM)]
        + [vmem] * len(arrays)
        + [pl.BlockSpec(memory_space=pl.ANY)] * len(apart),
        out_specs=tuple(vmem for _ in out_shape),
        scratch_shapes=list(scratch),
        cost_estimate=pl.CostEstimate(flops=flops, bytes_accessed=8 << 20, transcendentals=0),
        compiler_params=pltpu.CompilerParams(vmem_limit_bytes=20 << 20),
    )(where, *arrays, *apart)


def shards(tokens, norm_gain, chosen, route_weight, gate_weight, up_weight, down_weight):
    tok_rows, width = tokens.shape
    experts, capacity = chosen.shape
    p = lax.axis_index("ep")
    y = lax.axis_index("y")
    c = lax.axis_index("c")
    block = width // 16
    piece = 2 * block
    quarter = 2 * piece
    half_rows = capacity // 2
    slots = 3 * tok_rows // 32
    mate = [(0, 1), (1, 0)]
    tp = ("y", "c")
    to_major, to_major_2 = [
        [(2 * i + j, 2 * ((i + k * (1 - 2 * j)) % 8) + j) for i in range(8) for j in range(2)]
        for k in (1, 2)
    ]
    to_minor, to_minor_2 = [
        [(target, source) for source, target in pairs] for pairs in (to_major, to_major_2)
    ]

    place = jnp.stack([y, 1 - 2 * c, p * tok_rows, c]).astype(I32)
    pick_token, sent = dispatch(tokens, norm_gain, chosen, place, slots)
    got = lax.all_to_all(sent.reshape(experts, slots, quarter), "ep", 0, 0, tiled=True)
    got = got.reshape(experts * slots, quarter)

    gate_w, up_w, down_w, _ = lax.optimization_barrier(
        (gate_weight[0], up_weight[0], down_weight[0], sent)
    )
    gate_m = lax.ppermute(gate_w, "c", mate)
    up_m = lax.ppermute(up_w, "c", mate)
    down_m = lax.ppermute(down_w, "c", mate)

    mine = lax.dynamic_index_in_dim(chosen, p, 0, keepdims=False)
    edges = jnp.arange(experts + 1, dtype=I32) * tok_rows
    src_edge = jnp.sum((mine[None, :] < edges[:, None]).astype(I32), axis=1)
    k_edge = lax.shift_right_logical(src_edge - c + 1, 1)
    k_slot = k_edge[:-1, None] + jnp.arange(slots, dtype=I32)[None, :]
    k_slot = jnp.where(k_slot < k_edge[1:, None], k_slot, half_rows).reshape(experts * slots)
    my_weight = lax.dynamic_index_in_dim(
        route_weight.reshape(half_rows, 2), c, 1, keepdims=True
    )

    k_row, k_column = k_slot.reshape(1, experts * slots), k_slot.reshape(experts * slots, 1)
    k_row, k_column, my_weight, got = lax.optimization_barrier((k_row, k_column, my_weight, got))
    mid = half_rows // 2
    mid_shape = jax.ShapeDtypeStruct((mid, quarter), BF16)
    own, own_a, own_b = call_vmem(
        own_kernel,
        [jax.ShapeDtypeStruct((half_rows, quarter), BF16), mid_shape, mid_shape],
        2 * half_rows * experts * slots * quarter,
        place,
        [k_row, got],
    )
    major_a = lax.ppermute(own_a, tp, to_major)
    minor_b = lax.ppermute(own_b, tp, to_minor)
    major_b = lax.ppermute(own_b, tp, to_major)
    minor_a = lax.ppermute(own_a, tp, to_minor)
    far_a = lax.ppermute(major_a, tp, to_major)
    far_b = lax.ppermute(minor_b, tp, to_minor)

    def view(w):
        return w.reshape(2, 4, piece, w.shape[1])

    units = gate_w.shape[1]
    *totals, far_rows = call_vmem(
        near_kernel,
        [jax.ShapeDtypeStruct((half_rows, units), F32)] * 4
        + [jax.ShapeDtypeStruct((4, 2, piece, units), BF16)],
        2 * half_rows * 3 * quarter * 4 * units,
        place,
        [own, major_a, major_b, minor_a, minor_b],
        [view(w) for w in (gate_w, up_w, gate_m, up_m)],
        [pltpu.VMEM((4, 3, 2, piece, units), BF16), pltpu.SemaphoreType.DMA((4, 4))],
    )
    hid_shape = jax.ShapeDtypeStruct((half_rows, units), BF16)
    first_shape = jax.ShapeDtypeStruct((mid, piece), BF16)
    hid, hid_m, first_a, first_b = call_vmem(
        far_kernel,
        [hid_shape, hid_shape, first_shape, first_shape],
        2 * half_rows * (quarter * 4 * units + 2 * units * piece),
        place,
        [far_a, far_b, *totals, far_rows, down_w, down_m],
    )

    def outs_at(offsets, dtype):
        return call_vmem(
            functools.partial(out_kernel, offsets),
            [jax.ShapeDtypeStruct((half_rows, piece), dtype)] * len(offsets),
            2 * half_rows * 2 * units * len(offsets) * piece,
            place,
            [hid, hid_m, down_w, down_m],
        )

    def passed(mine, received):
        return (mine + received.astype(F32)).astype(BF16)

    jump_major = lax.ppermute(first_a, tp, to_major_2)
    jump_minor = lax.ppermute(first_b, tp, to_minor_2)
    major_3, minor_3 = outs_at((3, -3), BF16)
    r_major = lax.ppermute(major_3, tp, to_major)
    r_minor = lax.ppermute(minor_3, tp, to_minor)
    major_2, minor_2 = outs_at((2, -2), F32)
    major_2 = major_2 + jnp.pad(jump_major.astype(F32), ((0, mid), (0, 0)))
    minor_2 = minor_2 + jnp.pad(jump_minor.astype(F32), ((mid, 0), (0, 0)))
    r_major = lax.ppermute(passed(major_2, r_major), tp, to_major)
    r_minor = lax.ppermute(passed(minor_2, r_minor), tp, to_minor)
    major_1, minor_1, own_out = outs_at((1, -1, 0), F32)
    r_major = lax.ppermute(passed(major_1, r_major), tp, to_major)
    r_minor = lax.ppermute(passed(minor_1, r_minor), tp, to_minor)
    (back,) = call_vmem(
        back_kernel,
        [jax.ShapeDtypeStruct((experts * slots, piece), BF16)],
        2 * experts * slots * half_rows * piece,
        place,
        [k_column, own_out, r_major, r_minor, my_weight],
    )
    back = back.reshape(experts, slots, piece)
    returned = lax.all_to_all(back, "ep", 0, 0, tiled=True).reshape(experts * slots, piece)
    part = dot(pick_token, returned, OVER_ROWS)

    other = lax.dynamic_slice_in_dim(part, (1 - c) * block, block, 1).astype(BF16)
    theirs = lax.ppermute(other, "c", mate)
    combined = lax.dynamic_slice_in_dim(part, c * block, block, 1) + theirs.astype(F32)
    return combined.astype(BF16)


def solution(mesh):
    finer = Mesh(mesh.devices.reshape(mesh.shape["ep"], 8, 2), ("ep", "y", "c"))
    tp = ("y", "c")
    in_specs = (
        P("ep", None),
        P(),
        P(),
        P("ep", None),
        P("ep", None, tp),
        P("ep", None, tp),
        P("ep", tp, None),
    )

    return jax.shard_map(
        shards, mesh=finer, in_specs=in_specs, out_specs=P("ep", tp), check_vma=False
    )
```

```python
import functools

import jax
import jax.numpy as jnp
from jax import lax
from jax.experimental import pallas as pl
from jax.experimental.pallas import tpu as pltpu
from jax.sharding import Mesh
from jax.sharding import PartitionSpec as P


BF16 = jnp.bfloat16
F32 = jnp.float32
I32 = jnp.int32
OVER_ROWS = (((0,), (0,)), ((), ()))


def dot(a, b, dims=(((1,), (0,)), ((), ()))):
    return lax.dot_general(a, b, dims, preferred_element_type=F32)


def dispatch_kernel(
    slots, where_ref, tokens_in, gain_in, chosen_in, pick_ref, sent_ref,
    held, tokens_ref, gain_ref, chosen_ref, sems,
):
    copies = [
        pltpu.make_async_copy(chosen_in, chosen_ref, sems.at[0]),
        pltpu.make_async_copy(tokens_in, tokens_ref, sems.at[1]),
        pltpu.make_async_copy(gain_in, gain_ref, sems.at[2]),
    ]
    for copy in copies:
        copy.start()
    copies[0].wait()
    tok_rows, width = tokens_ref.shape
    experts, capacity = chosen_ref.shape
    q, first_token, parity = where_ref[0] & 3, where_ref[1], where_ref[2]
    chosen = chosen_ref[...]
    run_start = jnp.sum((chosen < first_token).astype(I32), axis=1, keepdims=True)
    run_end = jnp.sum((chosen < first_token + tok_rows).astype(I32), axis=1, keepdims=True)
    first = run_start + ((run_start + parity) & 1)
    rank = lax.broadcasted_iota(I32, (slots, capacity), 1)
    step = 2 * lax.broadcasted_iota(I32, (slots, capacity), 0)
    ahead = rank - step
    slot = 2 * lax.broadcasted_iota(I32, (slots, 1), 0)
    column = lax.broadcasted_iota(I32, (slots, tok_rows), 1)
    for e in range(experts):
        start = first[e : e + 1, :]
        token = jnp.sum(
            jnp.where(ahead == start, chosen[e : e + 1, :], 0), axis=1, keepdims=True
        )
        local = jnp.where(slot + start < run_end[e : e + 1, :], token - first_token, tok_rows)
        held[e * slots : (e + 1) * slots, :] = (column == local).astype(F32)
    copies[1].wait()
    copies[2].wait()
    values = tokens_ref[...].astype(F32)
    scale = lax.rsqrt(jnp.mean(values * values, axis=-1, keepdims=True) + 1e-06)
    piece = width // 8
    pick = held[...].astype(BF16)
    pick_ref[...] = pick
    for s in range(2):
        at = pl.multiple_of(s * (width // 2) + q * piece, piece)
        part = tokens_ref[:, pl.ds(at, piece)].astype(F32)
        normed = (part * scale * gain_ref[:, pl.ds(at, piece)]).astype(BF16)
        sent_ref[:, s * piece : (s + 1) * piece] = jnp.dot(
            pick, normed, preferred_element_type=F32
        ).astype(BF16)


def dispatch(tokens, norm_gain, chosen, where, slots):
    experts = chosen.shape[0]
    tok_rows, width = tokens.shape
    rows = experts * slots
    vmem = pl.BlockSpec(memory_space=pltpu.VMEM)
    return pl.pallas_call(
        functools.partial(dispatch_kernel, slots),
        out_shape=(
            jax.ShapeDtypeStruct((rows, tok_rows), BF16),
            jax.ShapeDtypeStruct((rows, width // 4), BF16),
        ),
        in_specs=[pl.BlockSpec(memory_space=pltpu.SMEM)] + [pl.BlockSpec(memory_space=pltpu.HBM)] * 3,
        out_specs=(vmem, vmem),
        scratch_shapes=[
            pltpu.VMEM((rows, tok_rows), F32),
            pltpu.VMEM((tok_rows, width), BF16),
            pltpu.VMEM((1, width), F32),
            pltpu.VMEM(chosen.shape, I32),
            pltpu.SemaphoreType.DMA((3,)),
        ],
        compiler_params=pltpu.CompilerParams(vmem_limit_bytes=60 << 20),
    )(where, tokens, norm_gain.reshape(1, width), chosen)


def flat(rows):
    return rows.reshape(rows.shape[0] * rows.shape[1], rows.shape[2])


def columns(ref, where_ref, k, piece):
    j = (where_ref[0] + k) & 7
    return ref[:, pl.ds(pl.multiple_of(j * piece, piece), piece)]


def near_kernel(where_ref, own, major_a, major_b, minor_a, minor_b, *refs):
    weights, totals, far_rows, held, sems = refs[:4], refs[4:8], refs[8], refs[9], refs[10]
    y = where_ref[0]
    quarters = (y & 3, (y + 3) & 3, (y + 1) & 3, (y + 2) & 3)
    copies = [
        [
            pltpu.make_async_copy(
                w.at[:, j], held.at[n, i] if i < 3 else far_rows.at[n], sems.at[n, i]
            )
            for i, j in enumerate(quarters)
        ]
        for n, w in enumerate(weights)
    ]
    for row in copies:
        for copy in row[:3]:
            copy.start()
    for row in copies:
        row[3].start()
    mid = major_a.shape[0]
    for n, total in enumerate(totals):
        for copy in copies[n][:3]:
            copy.wait()
        w_own, w_major, w_minor = [flat(held[n, i]) for i in range(3)]
        for r, (major, minor) in enumerate(((major_a, minor_a), (major_b, minor_b))):
            rows = slice(r * mid, (r + 1) * mid)
            total[rows, :] = (
                dot(own[rows, :], w_own) + dot(major[...], w_major) + dot(minor[...], w_minor)
            )
    for row in copies:
        row[3].wait()


def far_kernel(
    where_ref, far_a, far_b, t_gate, t_up, t_gate_m, t_up_m, far_rows, down, down_m,
    hid, hid_m, first_a, first_b,
):
    mid, piece = first_a.shape
    d_own = columns(down, where_ref, 4, piece)
    d_mate = columns(down_m, where_ref, 4, piece)
    w = [flat(far_rows[n]) for n in range(4)]
    for r, (far, first) in enumerate(((far_a, first_a), (far_b, first_b))):
        rows = slice(r * mid, (r + 1) * mid)

        def gated(t_g, t_u, w_g, w_u):
            g = t_g[rows, :] + dot(far[...], w_g)
            u = t_u[rows, :] + dot(far[...], w_u)
            return (g / (1.0 + jnp.exp(-g)) * u).astype(BF16)

        h_own = gated(t_gate, t_up, w[0], w[1])
        h_mate = gated(t_gate_m, t_up_m, w[2], w[3])
        hid[rows, :] = h_own
        hid_m[rows, :] = h_mate
        first[...] = (dot(h_own, d_own) + dot(h_mate, d_mate)).astype(first.dtype)


def out_kernel(offsets, where_ref, hid, hid_m, down, down_m, *outs):
    piece = outs[0].shape[1]
    for k, out in zip(offsets, outs):
        value = dot(hid[...], columns(down, where_ref, k, piece))
        value = value + dot(hid_m[...], columns(down_m, where_ref, k, piece))
        out[...] = value.astype(out.dtype)


def own_kernel(where_ref, k_slot, got, own, own_a, own_b):
    row = lax.broadcasted_iota(I32, (own.shape[0], got.shape[0]), 0)
    pick = (row == k_slot[...]).astype(F32).astype(BF16)
    rows = dot(pick, got[...]).astype(BF16)
    mid = own_a.shape[0]
    own[...] = rows
    own_a[...] = rows[:mid, :]
    own_b[...] = rows[mid:, :]


def back_kernel(where_ref, k_slot, own, r_major, r_minor, weight, back):
    row = lax.broadcasted_iota(I32, (back.shape[0], own.shape[0]), 1)
    pick = (row == k_slot[...]).astype(F32).astype(BF16)
    total = own[...] + r_major[...].astype(F32) + r_minor[...].astype(F32)
    weighted = (total * weight[...]).astype(BF16)
    back[...] = dot(pick, weighted).astype(BF16)


def call_vmem(kernel, out_shape, flops, where, arrays, apart=(), scratch=()):
    vmem = pl.BlockSpec(memory_space=pltpu.VMEM)
    return pl.pallas_call(
        kernel,
        out_shape=out_shape,
        in_specs=[pl.BlockSpec(memory_space=pltpu.SMEM)]
        + [vmem] * len(arrays)
        + [pl.BlockSpec(memory_space=pl.ANY)] * len(apart),
        out_specs=tuple(vmem for _ in out_shape),
        scratch_shapes=list(scratch),
        cost_estimate=pl.CostEstimate(flops=flops, bytes_accessed=8 << 20, transcendentals=0),
        compiler_params=pltpu.CompilerParams(vmem_limit_bytes=20 << 20),
    )(where, *arrays, *apart)


def shards(tokens, norm_gain, chosen, route_weight, gate_weight, up_weight, down_weight):
    tok_rows, width = tokens.shape
    experts, capacity = chosen.shape
    p = lax.axis_index("ep")
    y = lax.axis_index("y")
    c = lax.axis_index("c")
    block = width // 16
    piece = 2 * block
    quarter = 2 * piece
    half_rows = capacity // 2
    slots = 3 * tok_rows // 32
    mate = [(0, 1), (1, 0)]
    tp = ("y", "c")
    to_major, to_major_2 = [
        [(2 * i + j, 2 * ((i + k) % 8) + j) for i in range(8) for j in range(2)]
        for k in (1, 2)
    ]
    to_minor, to_minor_2 = [
        [(target, source) for source, target in pairs] for pairs in (to_major, to_major_2)
    ]

    place = jnp.stack([y, p * tok_rows, c]).astype(I32)
    pick_token, sent = dispatch(tokens, norm_gain, chosen, place, slots)
    got = lax.all_to_all(sent.reshape(experts, slots, quarter), "ep", 0, 0, tiled=True)
    got = got.reshape(experts * slots, quarter)

    gate_w, up_w, down_w, _ = lax.optimization_barrier(
        (gate_weight[0], up_weight[0], down_weight[0], sent)
    )
    gate_m = lax.ppermute(gate_w, "c", mate)
    up_m = lax.ppermute(up_w, "c", mate)
    down_m = lax.ppermute(down_w, "c", mate)

    mine = lax.dynamic_index_in_dim(chosen, p, 0, keepdims=False)
    edges = jnp.arange(experts + 1, dtype=I32) * tok_rows
    src_edge = jnp.sum((mine[None, :] < edges[:, None]).astype(I32), axis=1)
    k_edge = lax.shift_right_logical(src_edge - c + 1, 1)
    k_slot = k_edge[:-1, None] + jnp.arange(slots, dtype=I32)[None, :]
    k_slot = jnp.where(k_slot < k_edge[1:, None], k_slot, half_rows).reshape(experts * slots)
    my_weight = lax.dynamic_index_in_dim(
        route_weight.reshape(half_rows, 2), c, 1, keepdims=True
    )

    k_row, k_column = k_slot.reshape(1, experts * slots), k_slot.reshape(experts * slots, 1)
    k_row, k_column, my_weight, got = lax.optimization_barrier((k_row, k_column, my_weight, got))
    mid = half_rows // 2
    mid_shape = jax.ShapeDtypeStruct((mid, quarter), BF16)
    own, own_a, own_b = call_vmem(
        own_kernel,
        [jax.ShapeDtypeStruct((half_rows, quarter), BF16), mid_shape, mid_shape],
        2 * half_rows * experts * slots * quarter,
        place,
        [k_row, got],
    )
    major_a = lax.ppermute(own_a, tp, to_major)
    minor_b = lax.ppermute(own_b, tp, to_minor)
    major_b = lax.ppermute(own_b, tp, to_major)
    minor_a = lax.ppermute(own_a, tp, to_minor)
    far_a = lax.ppermute(major_a, tp, to_major)
    far_b = lax.ppermute(minor_b, tp, to_minor)

    def view(w):
        return w.reshape(2, 4, piece, w.shape[1])

    units = gate_w.shape[1]
    *totals, far_rows = call_vmem(
        near_kernel,
        [jax.ShapeDtypeStruct((half_rows, units), F32)] * 4
        + [jax.ShapeDtypeStruct((4, 2, piece, units), BF16)],
        2 * half_rows * 3 * quarter * 4 * units,
        place,
        [own, major_a, major_b, minor_a, minor_b],
        [view(w) for w in (gate_w, up_w, gate_m, up_m)],
        [pltpu.VMEM((4, 3, 2, piece, units), BF16), pltpu.SemaphoreType.DMA((4, 4))],
    )
    hid_shape = jax.ShapeDtypeStruct((half_rows, units), BF16)
    first_shape = jax.ShapeDtypeStruct((mid, piece), BF16)
    hid, hid_m, first_a, first_b = call_vmem(
        far_kernel,
        [hid_shape, hid_shape, first_shape, first_shape],
        2 * half_rows * (quarter * 4 * units + 2 * units * piece),
        place,
        [far_a, far_b, *totals, far_rows, down_w, down_m],
    )

    def outs_at(offsets, dtype):
        return call_vmem(
            functools.partial(out_kernel, offsets),
            [jax.ShapeDtypeStruct((half_rows, piece), dtype)] * len(offsets),
            2 * half_rows * 2 * units * len(offsets) * piece,
            place,
            [hid, hid_m, down_w, down_m],
        )

    def passed(mine, received):
        return (mine + received.astype(F32)).astype(BF16)

    jump_major = lax.ppermute(first_a, tp, to_major_2)
    jump_minor = lax.ppermute(first_b, tp, to_minor_2)
    major_3, minor_3 = outs_at((3, -3), BF16)
    r_major = lax.ppermute(major_3, tp, to_major)
    r_minor = lax.ppermute(minor_3, tp, to_minor)
    major_2, minor_2 = outs_at((2, -2), F32)
    major_2 = major_2 + jnp.pad(jump_major.astype(F32), ((0, mid), (0, 0)))
    minor_2 = minor_2 + jnp.pad(jump_minor.astype(F32), ((mid, 0), (0, 0)))
    r_major = lax.ppermute(passed(major_2, r_major), tp, to_major)
    r_minor = lax.ppermute(passed(minor_2, r_minor), tp, to_minor)
    major_1, minor_1, own_out = outs_at((1, -1, 0), F32)
    r_major = lax.ppermute(passed(major_1, r_major), tp, to_major)
    r_minor = lax.ppermute(passed(minor_1, r_minor), tp, to_minor)
    (back,) = call_vmem(
        back_kernel,
        [jax.ShapeDtypeStruct((experts * slots, piece), BF16)],
        2 * experts * slots * half_rows * piece,
        place,
        [k_column, own_out, r_major, r_minor, my_weight],
    )
    back = back.reshape(experts, slots, piece)
    returned = lax.all_to_all(back, "ep", 0, 0, tiled=True).reshape(experts * slots, piece)
    part = dot(pick_token, returned, OVER_ROWS)

    other = lax.dynamic_slice_in_dim(part, (1 - c) * block, block, 1).astype(BF16)
    theirs = lax.ppermute(other, "c", mate)
    combined = lax.dynamic_slice_in_dim(part, c * block, block, 1) + theirs.astype(F32)
    return combined.astype(BF16)


def solution(mesh):
    finer = Mesh(mesh.devices.reshape(mesh.shape["ep"], 8, 2), ("ep", "y", "c"))
    tp = ("y", "c")
    in_specs = (
        P("ep", None),
        P(),
        P(),
        P("ep", None),
        P("ep", None, tp),
        P("ep", None, tp),
        P("ep", tp, None),
    )

    return jax.shard_map(
        shards, mesh=finer, in_specs=in_specs, out_specs=P("ep", tp), check_vma=False
    )
```

```python
import functools

import jax
import jax.numpy as jnp
from jax import lax
from jax.experimental import pallas as pl
from jax.experimental.pallas import tpu as pltpu
from jax.sharding import Mesh
from jax.sharding import PartitionSpec as P


BF16 = jnp.bfloat16
F32 = jnp.float32
I32 = jnp.int32
OVER_ROWS = (((0,), (0,)), ((), ()))


def dot(a, b, dims=(((1,), (0,)), ((), ()))):
    return lax.dot_general(a, b, dims, preferred_element_type=F32)


def dispatch_kernel(
    slots, tokens_in, gain_in, chosen_in, pick_ref, sent_ref,
    held, tokens_ref, gain_ref, chosen_ref, sems,
):
    copies = [
        pltpu.make_async_copy(chosen_in, chosen_ref, sems.at[0]),
        pltpu.make_async_copy(tokens_in, tokens_ref, sems.at[1]),
        pltpu.make_async_copy(gain_in, gain_ref, sems.at[2]),
    ]
    for copy in copies:
        copy.start()
    copies[0].wait()
    tok_rows, width = tokens_ref.shape
    experts, capacity = chosen_ref.shape
    q, parity = lax.axis_index("y") & 3, lax.axis_index("c")
    first_token = lax.axis_index("ep") * tok_rows
    chosen = chosen_ref[...]
    run_start = jnp.sum((chosen < first_token).astype(I32), axis=1, keepdims=True)
    run_end = jnp.sum((chosen < first_token + tok_rows).astype(I32), axis=1, keepdims=True)
    first = run_start + ((run_start + parity) & 1)
    rank = lax.broadcasted_iota(I32, (slots, capacity), 1)
    step = 2 * lax.broadcasted_iota(I32, (slots, capacity), 0)
    ahead = rank - step
    slot = 2 * lax.broadcasted_iota(I32, (slots, 1), 0)
    column = lax.broadcasted_iota(I32, (slots, tok_rows), 1)
    for e in range(experts):
        start = first[e : e + 1, :]
        token = jnp.sum(
            jnp.where(ahead == start, chosen[e : e + 1, :], 0), axis=1, keepdims=True
        )
        local = jnp.where(slot + start < run_end[e : e + 1, :], token - first_token, tok_rows)
        held[e * slots : (e + 1) * slots, :] = (column == local).astype(F32)
    copies[1].wait()
    copies[2].wait()
    values = tokens_ref[...].astype(F32)
    scale = lax.rsqrt(jnp.mean(values * values, axis=-1, keepdims=True) + 1e-06)
    piece = width // 8
    pick = held[...].astype(BF16)
    pick_ref[...] = pick
    for s in range(2):
        at = pl.multiple_of(s * (width // 2) + q * piece, piece)
        part = tokens_ref[:, pl.ds(at, piece)].astype(F32)
        normed = (part * scale * gain_ref[:, pl.ds(at, piece)]).astype(BF16)
        sent_ref[:, s * piece : (s + 1) * piece] = jnp.dot(
            pick, normed, preferred_element_type=F32
        ).astype(BF16)


def dispatch(tokens, norm_gain, chosen, slots):
    experts = chosen.shape[0]
    tok_rows, width = tokens.shape
    rows = experts * slots
    vmem = pl.BlockSpec(memory_space=pltpu.VMEM)
    return pl.pallas_call(
        functools.partial(dispatch_kernel, slots),
        out_shape=(
            jax.ShapeDtypeStruct((rows, tok_rows), BF16),
            jax.ShapeDtypeStruct((rows, width // 4), BF16),
        ),
        in_specs=[pl.BlockSpec(memory_space=pltpu.HBM)] * 3,
        out_specs=(vmem, vmem),
        scratch_shapes=[
            pltpu.VMEM((rows, tok_rows), F32),
            pltpu.VMEM((tok_rows, width), BF16),
            pltpu.VMEM((1, width), F32),
            pltpu.VMEM(chosen.shape, I32),
            pltpu.SemaphoreType.DMA((3,)),
        ],
        compiler_params=pltpu.CompilerParams(vmem_limit_bytes=60 << 20),
    )(tokens, norm_gain.reshape(1, width), chosen)


def flat(rows):
    return rows.reshape(rows.shape[0] * rows.shape[1], rows.shape[2])


def columns(ref, where_ref, k, piece):
    j = (where_ref[0] + k) & 7
    return ref[:, pl.ds(pl.multiple_of(j * piece, piece), piece)]


def near_kernel(where_ref, own, major_a, major_b, minor_a, minor_b, *refs):
    weights, totals, far_rows, held, sems = refs[:4], refs[4:8], refs[8], refs[9], refs[10]
    y = where_ref[0]
    quarters = (y & 3, (y + 3) & 3, (y + 1) & 3, (y + 2) & 3)
    copies = [
        [
            pltpu.make_async_copy(
                w.at[:, j], held.at[n, i] if i < 3 else far_rows.at[n], sems.at[n, i]
            )
            for i, j in enumerate(quarters)
        ]
        for n, w in enumerate(weights)
    ]
    for row in copies:
        for copy in row[:3]:
            copy.start()
    for row in copies:
        row[3].start()
    mid = major_a.shape[0]
    for n, total in enumerate(totals):
        for copy in copies[n][:3]:
            copy.wait()
        w_own, w_major, w_minor = [flat(held[n, i]) for i in range(3)]
        for r, (major, minor) in enumerate(((major_a, minor_a), (major_b, minor_b))):
            rows = slice(r * mid, (r + 1) * mid)
            total[rows, :] = (
                dot(own[rows, :], w_own) + dot(major[...], w_major) + dot(minor[...], w_minor)
            )
    for row in copies:
        row[3].wait()


def far_kernel(
    where_ref, far_a, far_b, t_gate, t_up, t_gate_m, t_up_m, far_rows, down, down_m,
    hid, hid_m, first,
):
    mid, piece = far_a.shape[0], first.shape[1]
    d_own = columns(down, where_ref, 4, piece)
    d_mate = columns(down_m, where_ref, 4, piece)
    w = [flat(far_rows[n]) for n in range(4)]
    for r, far in enumerate((far_a, far_b)):
        rows = slice(r * mid, (r + 1) * mid)

        def gated(t_g, t_u, w_g, w_u):
            g = t_g[rows, :] + dot(far[...], w_g)
            u = t_u[rows, :] + dot(far[...], w_u)
            return (g / (1.0 + jnp.exp(-g)) * u).astype(BF16)

        h_own = gated(t_gate, t_up, w[0], w[1])
        h_mate = gated(t_gate_m, t_up_m, w[2], w[3])
        hid[rows, :] = h_own
        hid_m[rows, :] = h_mate
        first[rows, :] = (dot(h_own, d_own) + dot(h_mate, d_mate)).astype(first.dtype)


def out_kernel(offsets, where_ref, hid, hid_m, down, down_m, *refs):
    outs = refs[-len(offsets) :]
    piece = outs[0].shape[1]
    for n, (k, out) in enumerate(zip(offsets, outs)):
        value = dot(hid[...], columns(down, where_ref, k, piece))
        value = value + dot(hid_m[...], columns(down_m, where_ref, k, piece))
        if len(refs) > len(offsets):
            value = value + jnp.where(lax.axis_index("c") == n, refs[0][...].astype(F32), 0.0)
        out[...] = value.astype(out.dtype)


def own_kernel(where_ref, k_slot, got, own, own_a, own_b):
    row = lax.broadcasted_iota(I32, (own.shape[0], got.shape[0]), 0)
    pick = (row == k_slot[...]).astype(F32).astype(BF16)
    rows = dot(pick, got[...]).astype(BF16)
    mid = own_a.shape[0]
    own[...] = rows
    own_a[...] = rows[:mid, :]
    own_b[...] = rows[mid:, :]


def back_kernel(where_ref, k_slot, own, r_major, r_minor, weight, back):
    row = lax.broadcasted_iota(I32, (back.shape[0], own.shape[0]), 1)
    pick = (row == k_slot[...]).astype(F32).astype(BF16)
    total = own[...] + r_major[...].astype(F32) + r_minor[...].astype(F32)
    weighted = (total * weight[...]).astype(BF16)
    back[...] = dot(pick, weighted).astype(BF16)


def call_vmem(kernel, out_shape, flops, where, arrays, apart=(), scratch=()):
    vmem = pl.BlockSpec(memory_space=pltpu.VMEM)
    return pl.pallas_call(
        kernel,
        out_shape=out_shape,
        in_specs=[pl.BlockSpec(memory_space=pltpu.SMEM)]
        + [vmem] * len(arrays)
        + [pl.BlockSpec(memory_space=pl.ANY)] * len(apart),
        out_specs=tuple(vmem for _ in out_shape),
        scratch_shapes=list(scratch),
        cost_estimate=pl.CostEstimate(flops=flops, bytes_accessed=8 << 20, transcendentals=0),
        compiler_params=pltpu.CompilerParams(vmem_limit_bytes=20 << 20),
    )(where, *arrays, *apart)


def shards(tokens, norm_gain, chosen, route_weight, gate_weight, up_weight, down_weight):
    tok_rows, width = tokens.shape
    experts, capacity = chosen.shape
    p = lax.axis_index("ep")
    y = lax.axis_index("y")
    c = lax.axis_index("c")
    block = width // 16
    piece = 2 * block
    quarter = 2 * piece
    half_rows = capacity // 2
    slots = 3 * tok_rows // 32
    mate = [(0, 1), (1, 0)]
    tp = ("y", "c")
    to_major = [(2 * i + j, 2 * ((i + 1) % 8) + j) for i in range(8) for j in range(2)]
    to_minor = [(target, source) for source, target in to_major]
    jumps = [(2 * i + j, 2 * ((i + 2 - 4 * j) % 8) + j) for i in range(8) for j in range(2)]

    place = y.astype(I32).reshape(1)
    pick_token, sent = dispatch(tokens, norm_gain, chosen, slots)
    got = lax.all_to_all(sent.reshape(experts, slots, quarter), "ep", 0, 0, tiled=True)
    got = got.reshape(experts * slots, quarter)

    gate_w, up_w, down_w, _ = lax.optimization_barrier(
        (gate_weight[0], up_weight[0], down_weight[0], sent)
    )
    gate_m = lax.ppermute(gate_w, "c", mate)
    up_m = lax.ppermute(up_w, "c", mate)
    down_m = lax.ppermute(down_w, "c", mate)

    mine = lax.dynamic_index_in_dim(chosen, p, 0, keepdims=False)
    edges = jnp.arange(experts + 1, dtype=I32) * tok_rows
    src_edge = jnp.sum((mine[None, :] < edges[:, None]).astype(I32), axis=1)
    k_edge = lax.shift_right_logical(src_edge - c + 1, 1)
    k_slot = k_edge[:-1, None] + jnp.arange(slots, dtype=I32)[None, :]
    k_slot = jnp.where(k_slot < k_edge[1:, None], k_slot, half_rows).reshape(experts * slots)
    my_weight = lax.dynamic_index_in_dim(
        route_weight.reshape(half_rows, 2), c, 1, keepdims=True
    )

    k_row, k_column = k_slot.reshape(1, experts * slots), k_slot.reshape(experts * slots, 1)
    k_row, k_column, my_weight, got = lax.optimization_barrier((k_row, k_column, my_weight, got))
    mid = half_rows // 2
    mid_shape = jax.ShapeDtypeStruct((mid, quarter), BF16)
    own, own_a, own_b = call_vmem(
        own_kernel,
        [jax.ShapeDtypeStruct((half_rows, quarter), BF16), mid_shape, mid_shape],
        2 * half_rows * experts * slots * quarter,
        place,
        [k_row, got],
    )
    major_a = lax.ppermute(own_a, tp, to_major)
    minor_b = lax.ppermute(own_b, tp, to_minor)
    major_b = lax.ppermute(own_b, tp, to_major)
    minor_a = lax.ppermute(own_a, tp, to_minor)
    far_a = lax.ppermute(major_a, tp, to_major)
    far_b = lax.ppermute(minor_b, tp, to_minor)

    def view(w):
        return w.reshape(2, 4, piece, w.shape[1])

    units = gate_w.shape[1]
    *totals, far_rows = call_vmem(
        near_kernel,
        [jax.ShapeDtypeStruct((half_rows, units), F32)] * 4
        + [jax.ShapeDtypeStruct((4, 2, piece, units), BF16)],
        2 * half_rows * 3 * quarter * 4 * units,
        place,
        [own, major_a, major_b, minor_a, minor_b],
        [view(w) for w in (gate_w, up_w, gate_m, up_m)],
        [pltpu.VMEM((4, 3, 2, piece, units), BF16), pltpu.SemaphoreType.DMA((4, 4))],
    )
    hid_shape = jax.ShapeDtypeStruct((half_rows, units), BF16)
    hid, hid_m, first = call_vmem(
        far_kernel,
        [hid_shape, hid_shape, jax.ShapeDtypeStruct((half_rows, piece), BF16)],
        2 * half_rows * (quarter * 4 * units + 2 * units * piece),
        place,
        [far_a, far_b, *totals, far_rows, down_w, down_m],
    )

    def outs_at(offsets, dtype, *more):
        return call_vmem(
            functools.partial(out_kernel, offsets),
            [jax.ShapeDtypeStruct((half_rows, piece), dtype)] * len(offsets),
            2 * half_rows * 2 * units * len(offsets) * piece,
            place,
            [hid, hid_m, down_w, down_m, *more],
        )

    def passed(mine, received):
        return (mine + received.astype(F32)).astype(BF16)

    jumped = lax.ppermute(first, tp, jumps)
    major_3, minor_3 = outs_at((3, -3), BF16)
    r_major = lax.ppermute(major_3, tp, to_major)
    r_minor = lax.ppermute(minor_3, tp, to_minor)
    major_2, minor_2 = outs_at((2, -2), F32, jumped)
    r_major = lax.ppermute(passed(major_2, r_major), tp, to_major)
    r_minor = lax.ppermute(passed(minor_2, r_minor), tp, to_minor)
    major_1, minor_1, own_out = outs_at((1, -1, 0), F32)
    r_major = lax.ppermute(passed(major_1, r_major), tp, to_major)
    r_minor = lax.ppermute(passed(minor_1, r_minor), tp, to_minor)
    (back,) = call_vmem(
        back_kernel,
        [jax.ShapeDtypeStruct((experts * slots, piece), BF16)],
        2 * experts * slots * half_rows * piece,
        place,
        [k_column, own_out, r_major, r_minor, my_weight],
    )
    back = back.reshape(experts, slots, piece)
    returned = lax.all_to_all(back, "ep", 0, 0, tiled=True).reshape(experts * slots, piece)
    part = dot(pick_token, returned, OVER_ROWS)

    other = lax.dynamic_slice_in_dim(part, (1 - c) * block, block, 1).astype(BF16)
    theirs = lax.ppermute(other, "c", mate)
    combined = lax.dynamic_slice_in_dim(part, c * block, block, 1) + theirs.astype(F32)
    return combined.astype(BF16)


def solution(mesh):
    finer = Mesh(mesh.devices.reshape(mesh.shape["ep"], 8, 2), ("ep", "y", "c"))
    tp = ("y", "c")
    in_specs = (
        P("ep", None),
        P(),
        P(),
        P("ep", None),
        P("ep", None, tp),
        P("ep", None, tp),
        P("ep", tp, None),
    )

    return jax.shard_map(
        shards, mesh=finer, in_specs=in_specs, out_specs=P("ep", tp), check_vma=False
    )
```

```python
import functools

import jax
import jax.numpy as jnp
from jax import lax
from jax.experimental import pallas as pl
from jax.experimental.pallas import tpu as pltpu
from jax.sharding import Mesh
from jax.sharding import PartitionSpec as P


BF16 = jnp.bfloat16
F32 = jnp.float32
I32 = jnp.int32
OVER_ROWS = (((0,), (0,)), ((), ()))


def dot(a, b, dims=(((1,), (0,)), ((), ()))):
    return lax.dot_general(a, b, dims, preferred_element_type=F32)


def dispatch_kernel(
    slots, tokens_in, gain_in, chosen_in, pick_ref, sent_ref,
    held, tokens_ref, gain_ref, chosen_ref, sems,
):
    copies = [
        pltpu.make_async_copy(chosen_in, chosen_ref, sems.at[0]),
        pltpu.make_async_copy(tokens_in, tokens_ref, sems.at[1]),
        pltpu.make_async_copy(gain_in, gain_ref, sems.at[2]),
    ]
    for copy in copies:
        copy.start()
    copies[0].wait()
    tok_rows, width = tokens_ref.shape
    experts, capacity = chosen_ref.shape
    q, parity = lax.axis_index("y") & 3, lax.axis_index("c")
    first_token = lax.axis_index("ep") * tok_rows
    chosen = chosen_ref[...]
    run_start = jnp.sum((chosen < first_token).astype(I32), axis=1, keepdims=True)
    run_end = jnp.sum((chosen < first_token + tok_rows).astype(I32), axis=1, keepdims=True)
    first = run_start + ((run_start + parity) & 1)
    rank = lax.broadcasted_iota(I32, (slots, capacity), 1)
    step = 2 * lax.broadcasted_iota(I32, (slots, capacity), 0)
    ahead = rank - step
    slot = 2 * lax.broadcasted_iota(I32, (slots, 1), 0)
    column = lax.broadcasted_iota(I32, (slots, tok_rows), 1)
    for e in range(experts):
        start = first[e : e + 1, :]
        token = jnp.sum(
            jnp.where(ahead == start, chosen[e : e + 1, :], 0), axis=1, keepdims=True
        )
        local = jnp.where(slot + start < run_end[e : e + 1, :], token - first_token, tok_rows)
        held[e * slots : (e + 1) * slots, :] = (column == local).astype(F32)
    copies[1].wait()
    copies[2].wait()
    values = tokens_ref[...].astype(F32)
    scale = lax.rsqrt(jnp.mean(values * values, axis=-1, keepdims=True) + 1e-06)
    piece = width // 8
    pick = held[...].astype(BF16)
    pick_ref[...] = pick
    for s in range(2):
        at = pl.multiple_of(s * (width // 2) + q * piece, piece)
        part = tokens_ref[:, pl.ds(at, piece)].astype(F32)
        normed = (part * scale * gain_ref[:, pl.ds(at, piece)]).astype(BF16)
        sent_ref[:, s * piece : (s + 1) * piece] = jnp.dot(
            pick, normed, preferred_element_type=F32
        ).astype(BF16)


def dispatch(tokens, norm_gain, chosen, slots):
    experts = chosen.shape[0]
    tok_rows, width = tokens.shape
    rows = experts * slots
    vmem = pl.BlockSpec(memory_space=pltpu.VMEM)
    return pl.pallas_call(
        functools.partial(dispatch_kernel, slots),
        out_shape=(
            jax.ShapeDtypeStruct((rows, tok_rows), BF16),
            jax.ShapeDtypeStruct((rows, width // 4), BF16),
        ),
        in_specs=[pl.BlockSpec(memory_space=pltpu.HBM)] * 3,
        out_specs=(vmem, vmem),
        scratch_shapes=[
            pltpu.VMEM((rows, tok_rows), F32),
            pltpu.VMEM((tok_rows, width), BF16),
            pltpu.VMEM((1, width), F32),
            pltpu.VMEM(chosen.shape, I32),
            pltpu.SemaphoreType.DMA((3,)),
        ],
        compiler_params=pltpu.CompilerParams(vmem_limit_bytes=60 << 20),
    )(tokens, norm_gain.reshape(1, width), chosen)


def flat(rows):
    return rows.reshape(rows.shape[0] * rows.shape[1], rows.shape[2])


def columns(ref, where_ref, k, piece):
    j = (where_ref[0] + k) & 7
    return ref[:, pl.ds(pl.multiple_of(j * piece, piece), piece)]


def near_kernel(where_ref, own, major_a, major_b, minor_a, minor_b, *refs):
    weights, totals, far_rows, held, sems = refs[:4], refs[4:8], refs[8], refs[9], refs[10]
    y = where_ref[0]
    quarters = (y & 3, (y + 3) & 3, (y + 1) & 3, (y + 2) & 3)
    copies = [
        [
            pltpu.make_async_copy(
                w.at[:, j], held.at[n, i] if i < 3 else far_rows.at[n], sems.at[n, i]
            )
            for i, j in enumerate(quarters)
        ]
        for n, w in enumerate(weights)
    ]
    for row in copies:
        for copy in row[:3]:
            copy.start()
    for row in copies:
        row[3].start()
    mid = major_a.shape[0]
    for n, total in enumerate(totals):
        for copy in copies[n][:3]:
            copy.wait()
        w_own, w_major, w_minor = [flat(held[n, i]) for i in range(3)]
        for r, (major, minor) in enumerate(((major_a, minor_a), (major_b, minor_b))):
            rows = slice(r * mid, (r + 1) * mid)
            total[rows, :] = (
                dot(own[rows, :], w_own) + dot(major[...], w_major) + dot(minor[...], w_minor)
            )
    for row in copies:
        row[3].wait()


def far_kernel(
    where_ref, far_a, far_b, t_gate, t_up, t_gate_m, t_up_m, far_rows, down, down_m,
    hid, hid_m, first_a, first_b,
):
    mid, piece = first_a.shape
    d_own = columns(down, where_ref, 4, piece)
    d_mate = columns(down_m, where_ref, 4, piece)
    w = [flat(far_rows[n]) for n in range(4)]
    for r, (far, first) in enumerate(((far_a, first_a), (far_b, first_b))):
        rows = slice(r * mid, (r + 1) * mid)

        def gated(t_g, t_u, w_g, w_u):
            g = t_g[rows, :] + dot(far[...], w_g)
            u = t_u[rows, :] + dot(far[...], w_u)
            return (g / (1.0 + jnp.exp(-g)) * u).astype(BF16)

        h_own = gated(t_gate, t_up, w[0], w[1])
        h_mate = gated(t_gate_m, t_up_m, w[2], w[3])
        hid[rows, :] = h_own
        hid_m[rows, :] = h_mate
        first[...] = (dot(h_own, d_own) + dot(h_mate, d_mate)).astype(first.dtype)


def out_kernel(offsets, where_ref, hid, hid_m, down, down_m, *outs):
    piece = outs[0].shape[1]
    for k, out in zip(offsets, outs):
        value = dot(hid[...], columns(down, where_ref, k, piece))
        value = value + dot(hid_m[...], columns(down_m, where_ref, k, piece))
        out[...] = value.astype(out.dtype)


def own_kernel(where_ref, k_slot, got, own, own_a, own_b):
    row = lax.broadcasted_iota(I32, (own.shape[0], got.shape[0]), 0)
    pick = (row == k_slot[...]).astype(F32).astype(BF16)
    rows = dot(pick, got[...]).astype(BF16)
    mid = own_a.shape[0]
    own[...] = rows
    own_a[...] = rows[:mid, :]
    own_b[...] = rows[mid:, :]


def back_kernel(where_ref, k_slot, own, r_major, r_minor, weight, back):
    row = lax.broadcasted_iota(I32, (back.shape[0], own.shape[0]), 1)
    pick = (row == k_slot[...]).astype(F32).astype(BF16)
    total = own[...] + r_major[...].astype(F32) + r_minor[...].astype(F32)
    weighted = (total * weight[...]).astype(BF16)
    back[...] = dot(pick, weighted).astype(BF16)


def call_vmem(kernel, out_shape, flops, where, arrays, apart=(), scratch=()):
    vmem = pl.BlockSpec(memory_space=pltpu.VMEM)
    return pl.pallas_call(
        kernel,
        out_shape=out_shape,
        in_specs=[pl.BlockSpec(memory_space=pltpu.SMEM)]
        + [vmem] * len(arrays)
        + [pl.BlockSpec(memory_space=pl.ANY)] * len(apart),
        out_specs=tuple(vmem for _ in out_shape),
        scratch_shapes=list(scratch),
        cost_estimate=pl.CostEstimate(flops=flops, bytes_accessed=8 << 20, transcendentals=0),
        compiler_params=pltpu.CompilerParams(vmem_limit_bytes=20 << 20),
    )(where, *arrays, *apart)


def shards(tokens, norm_gain, chosen, route_weight, gate_weight, up_weight, down_weight):
    tok_rows, width = tokens.shape
    experts, capacity = chosen.shape
    p = lax.axis_index("ep")
    y = lax.axis_index("y")
    c = lax.axis_index("c")
    block = width // 16
    piece = 2 * block
    quarter = 2 * piece
    half_rows = capacity // 2
    slots = 3 * tok_rows // 32
    mate = [(0, 1), (1, 0)]
    tp = ("y", "c")
    to_major, to_major_2 = [
        [(2 * i + j, 2 * ((i + k) % 8) + j) for i in range(8) for j in range(2)]
        for k in (1, 2)
    ]
    to_minor, to_minor_2 = [
        [(target, source) for source, target in pairs] for pairs in (to_major, to_major_2)
    ]

    place = y.astype(I32).reshape(1)
    pick_token, sent = dispatch(tokens, norm_gain, chosen, slots)
    got = lax.all_to_all(sent.reshape(experts, slots, quarter), "ep", 0, 0, tiled=True)
    got = got.reshape(experts * slots, quarter)

    gate_w, up_w, down_w, _ = lax.optimization_barrier(
        (gate_weight[0], up_weight[0], down_weight[0], sent)
    )
    gate_m = lax.ppermute(gate_w, "c", mate)
    up_m = lax.ppermute(up_w, "c", mate)
    down_m = lax.ppermute(down_w, "c", mate)

    mine = lax.dynamic_index_in_dim(chosen, p, 0, keepdims=False)
    edges = jnp.arange(experts + 1, dtype=I32) * tok_rows
    src_edge = jnp.sum((mine[None, :] < edges[:, None]).astype(I32), axis=1)
    k_edge = lax.shift_right_logical(src_edge - c + 1, 1)
    k_slot = k_edge[:-1, None] + jnp.arange(slots, dtype=I32)[None, :]
    k_slot = jnp.where(k_slot < k_edge[1:, None], k_slot, half_rows).reshape(experts * slots)
    my_weight = lax.dynamic_index_in_dim(
        route_weight.reshape(half_rows, 2), c, 1, keepdims=True
    )

    k_row, k_column = k_slot.reshape(1, experts * slots), k_slot.reshape(experts * slots, 1)
    k_row, k_column, my_weight, got = lax.optimization_barrier((k_row, k_column, my_weight, got))
    mid = half_rows // 2
    mid_shape = jax.ShapeDtypeStruct((mid, quarter), BF16)
    own, own_a, own_b = call_vmem(
        own_kernel,
        [jax.ShapeDtypeStruct((half_rows, quarter), BF16), mid_shape, mid_shape],
        2 * half_rows * experts * slots * quarter,
        place,
        [k_row, got],
    )
    major_a = lax.ppermute(own_a, tp, to_major)
    minor_b = lax.ppermute(own_b, tp, to_minor)
    major_b = lax.ppermute(own_b, tp, to_major)
    minor_a = lax.ppermute(own_a, tp, to_minor)
    far_a = lax.ppermute(major_a, tp, to_major)
    far_b = lax.ppermute(minor_b, tp, to_minor)

    def view(w):
        return w.reshape(2, 4, piece, w.shape[1])

    units = gate_w.shape[1]
    *totals, far_rows = call_vmem(
        near_kernel,
        [jax.ShapeDtypeStruct((half_rows, units), F32)] * 4
        + [jax.ShapeDtypeStruct((4, 2, piece, units), BF16)],
        2 * half_rows * 3 * quarter * 4 * units,
        place,
        [own, major_a, major_b, minor_a, minor_b],
        [view(w) for w in (gate_w, up_w, gate_m, up_m)],
        [pltpu.VMEM((4, 3, 2, piece, units), BF16), pltpu.SemaphoreType.DMA((4, 4))],
    )
    hid_shape = jax.ShapeDtypeStruct((half_rows, units), BF16)
    first_shape = jax.ShapeDtypeStruct((mid, piece), BF16)
    hid, hid_m, first_a, first_b = call_vmem(
        far_kernel,
        [hid_shape, hid_shape, first_shape, first_shape],
        2 * half_rows * (quarter * 4 * units + 2 * units * piece),
        place,
        [far_a, far_b, *totals, far_rows, down_w, down_m],
    )

    def outs_at(offsets, dtype):
        return call_vmem(
            functools.partial(out_kernel, offsets),
            [jax.ShapeDtypeStruct((half_rows, piece), dtype)] * len(offsets),
            2 * half_rows * 2 * units * len(offsets) * piece,
            place,
            [hid, hid_m, down_w, down_m],
        )

    def passed(mine, received):
        return (mine + received.astype(F32)).astype(BF16)

    jump_major = lax.ppermute(first_a, tp, to_major_2)
    jump_minor = lax.ppermute(first_b, tp, to_minor_2)
    major_3, minor_3 = outs_at((3, -3), BF16)
    r_major = lax.ppermute(major_3, tp, to_major)
    r_minor = lax.ppermute(minor_3, tp, to_minor)
    major_2, minor_2 = outs_at((2, -2), F32)
    major_2 = major_2 + jnp.pad(jump_major.astype(F32), ((0, mid), (0, 0)))
    minor_2 = minor_2 + jnp.pad(jump_minor.astype(F32), ((mid, 0), (0, 0)))
    r_major = lax.ppermute(passed(major_2, r_major), tp, to_major)
    r_minor = lax.ppermute(passed(minor_2, r_minor), tp, to_minor)
    major_1, minor_1, own_out = outs_at((1, -1, 0), F32)
    r_major = lax.ppermute(passed(major_1, r_major), tp, to_major)
    r_minor = lax.ppermute(passed(minor_1, r_minor), tp, to_minor)
    (back,) = call_vmem(
        back_kernel,
        [jax.ShapeDtypeStruct((experts * slots, piece), BF16)],
        2 * experts * slots * half_rows * piece,
        place,
        [k_column, own_out, r_major, r_minor, my_weight],
    )
    back = back.reshape(experts, slots, piece)
    returned = lax.all_to_all(back, "ep", 0, 0, tiled=True).reshape(experts * slots, piece)
    part = dot(pick_token, returned, OVER_ROWS)

    other = lax.dynamic_slice_in_dim(part, (1 - c) * block, block, 1).astype(BF16)
    theirs = lax.ppermute(other, "c", mate)
    combined = lax.dynamic_slice_in_dim(part, c * block, block, 1) + theirs.astype(F32)
    return combined.astype(BF16)


def solution(mesh):
    finer = Mesh(mesh.devices.reshape(mesh.shape["ep"], 8, 2), ("ep", "y", "c"))
    tp = ("y", "c")
    in_specs = (
        P("ep", None),
        P(),
        P(),
        P("ep", None),
        P("ep", None, tp),
        P("ep", None, tp),
        P("ep", tp, None),
    )

    return jax.shard_map(
        shards, mesh=finer, in_specs=in_specs, out_specs=P("ep", tp), check_vma=False
    )
```
